32 devices in a mesh: kv: 8 (over z, y), tp: 4 (over x, core).
Axes of the slice: x: 2, y: 2, z: 4, core: 2. Of those that a mesh axis runs over, the one named last changes fastest.
Arguments:
- tokens: bfloat16 [2048, 4096], P('kv'), may hold values from -6 to 6
- norm_gain: float32 [4096], replicated, may hold values from 0.1 to 1.9
- w_query: bfloat16 [4096, 2048], P('kv', 'tp'), may hold values from -0.09375 to 0.09375
- w_forget: bfloat16 [4096, 2048], P('kv', 'tp'), may hold values from -0.09375 to 0.09375
- w_value: bfloat16 [4096, 2048], P('kv', 'tp'), may hold values from -0.09375 to 0.09375
- w_gate: bfloat16 [4096, 2048], P('kv', 'tp'), may hold values from -0.09375 to 0.09375
- lower_bound: float32 [2048], P('tp'), may hold values from 0 to 0.9
- head_gain: float32 [2048], P('tp'), may hold values from 0.1 to 1.9
- w_out: bfloat16 [2048, 4096], P('kv', 'tp'), may hold values from -0.125 to 0.125
- state: float32 [512, 16, 128, 128], P('kv', 'tp'), may hold values from -4 to 4
- prev_forget: bfloat16 [512, 4, 2048], P('kv', None, 'tp'), may hold values from -8 to 8
- prev_value: bfloat16 [512, 4, 2048], P('kv', None, 'tp'), may hold values from -6 to 6
- accepted: int32 [512], P('kv'), may hold values from 0 to 4
Outputs:
- mixed: bfloat16 [2048, 4096], P('kv', 'tp')
- taken_state: float32 [512, 16, 128, 128], P('kv', 'tp')
The draws below stay inside these ranges and needn't reach their ends.
All inputs are finite; a program needn't handle non-finite values.
Results may differ from the reference program's by a relative error of at most 0.015.
Values may be sent and summed in bfloat16 or wider, within the bound.
No kernel may reach another device: no remote copies, remote signals or barrier semaphores. Data moves between devices by JAX's collectives and lax.ppermute only.
A program may use at most 128 MiB of HBM per device.

```python
import jax
import jax.numpy as jnp
from jax import lax

D = 4096
HEADS = 16
KEY_DIM = 128
VAL_DIM = 128
PROPOSALS = 4
SEQS = 512
TOKENS = 2048
WIDTH = 2048


def with_ends(entries, own_key, least, largest):
    longest = entries.shape.index(max(entries.shape))
    spots = []
    for shift in (0, 1):
        where = [jax.random.randint(jax.random.fold_in(own_key, axis), (), 0, length) for axis, length in enumerate(entries.shape)]
        where[longest] = (where[longest] + shift) % entries.shape[longest]
        spots.append(tuple(where))
    return entries.at[spots[0]].set(least).at[spots[1]].set(largest)


def steps_of(own_key, extent, split, smallest, top_value):
    loudness, own = 1.0, jax.random.fold_in(own_key, 6)
    for axis_at, shards_of in split:
        heights = jnp.exp(jax.random.uniform(jax.random.fold_in(own, axis_at), (shards_of,), jnp.float32, smallest / len(split), top_value / len(split)))
        loudness = loudness * jnp.repeat(heights, extent[axis_at] // shards_of).reshape([-1 if axis == axis_at else 1 for axis in range(len(extent))])
    return loudness


def bell_draw(key, shape, width, reach, shards=(), kind=jnp.bfloat16):
    loudness = steps_of(key, shape, shards, -0.22, 0.18) if shards else 1.0
    result = jax.random.normal(key, shape, jnp.float32) * width * loudness
    return jnp.minimum(jnp.maximum(result, -reach), reach).astype(kind)


def setup_inputs(seed: int = 0) -> dict:
    key_of = jax.random.split(jax.random.key(seed), 14)
    return {
        "tokens": bell_draw(key_of[0], (TOKENS, D), 1.0, 6.0, ((0, 8),)),
        "norm_gain": jnp.clip(1.0 + 0.18 * jax.random.normal(key_of[1], (D,), jnp.float32), 0.1, 1.9),
        "w_query": bell_draw(key_of[2], (D, WIDTH), D ** -0.5, 0.09375, ((0, 8), (1, 4))),
        "w_forget": bell_draw(key_of[3], (D, WIDTH), D ** -0.5, 0.09375, ((0, 8), (1, 4))),
        "w_value": bell_draw(key_of[4], (D, WIDTH), D ** -0.5, 0.09375, ((0, 8), (1, 4))),
        "w_gate": bell_draw(key_of[5], (D, WIDTH), D ** -0.5, 0.09375, ((0, 8), (1, 4))),
        "lower_bound": jnp.clip(0.9 * jax.random.uniform(key_of[6], (WIDTH,), jnp.float32) ** steps_of(key_of[6], (WIDTH,), ((0, 4),), -0.2, 0.2), 0.0, 0.9),
        "head_gain": jnp.clip(1.0 + 0.18 * jax.random.normal(key_of[7], (WIDTH,), jnp.float32), 0.1, 1.9),
        "w_out": bell_draw(key_of[8], (WIDTH, D), WIDTH ** -0.5, 0.125, ((0, 8), (1, 4))),
        "state": bell_draw(key_of[9], (SEQS, HEADS, KEY_DIM, VAL_DIM), 0.5, 4.0, ((0, 8), (1, 4)), jnp.float32),
        "prev_forget": bell_draw(key_of[10], (SEQS, PROPOSALS, WIDTH), 1.5, 8.0, ((0, 8), (2, 4))),
        "prev_value": bell_draw(key_of[11], (SEQS, PROPOSALS, WIDTH), 1.0, 6.0, ((0, 8), (2, 4))),
        "accepted": with_ends(jax.random.randint(key_of[12], (SEQS,), 0, PROPOSALS + 1), jax.random.fold_in(key_of[12], 1), 0, PROPOSALS).astype(jnp.int32),
    }


EPSILON = 1e-06

def forget_of(pre_act, bounds):
    return bounds + (1.0 - bounds) * jax.nn.sigmoid(pre_act.astype(jnp.float32))

def recur_one(start_state, old_forget, old_values, accepted_count, queries, forget, new_values):
    carried = start_state
    for position in range(old_forget.shape[0]):
        kept_mask = position < accepted_count
        decay_rate = jnp.where(kept_mask, old_forget[position], 1.0)
        weight = jnp.where(kept_mask, 1.0 - old_forget[position], 0.0)
        carried = decay_rate[:, :, None] * carried + weight[:, :, None] * old_values[position][:, None, :]
    taken = carried
    outputs = []
    for position in range(queries.shape[0]):
        carried = forget[position][:, :, None] * carried + (1.0 - forget[position])[:, :, None] * new_values[position][:, None, :]
        outputs.append(jnp.einsum('hd,hde->he', queries[position], carried, precision=lax.Precision.HIGHEST))
    return (taken, jnp.stack(outputs))

def finish(outputs, head_gain, gate_proj):
    scaled = outputs * lax.rsqrt(lax.optimization_barrier(jnp.mean(outputs * outputs, axis=-1, keepdims=True)) + EPSILON)
    flat = scaled.reshape(gate_proj.shape)
    return (flat * head_gain * jax.nn.silu(gate_proj.astype(jnp.float32))).astype(jnp.bfloat16)

def reference(tokens, norm_gain, w_query, w_forget, w_value, w_gate, lower_bound, head_gain, w_out, state, prev_forget, prev_value, accepted):
    floated = tokens.astype(jnp.float32)
    normed = (floated * lax.rsqrt(lax.optimization_barrier(jnp.mean(floated * floated, axis=-1, keepdims=True)) + EPSILON) * norm_gain).astype(jnp.bfloat16)
    query_proj = jnp.dot(normed, w_query, preferred_element_type=jnp.float32).astype(jnp.bfloat16)
    forget_proj = jnp.dot(normed, w_forget, preferred_element_type=jnp.float32).astype(jnp.bfloat16)
    value_proj = jnp.dot(normed, w_value, preferred_element_type=jnp.float32).astype(jnp.bfloat16)
    gate_proj = jnp.dot(normed, w_gate, preferred_element_type=jnp.float32).astype(jnp.bfloat16)
    seq_total = state.shape[0]
    bounds = lower_bound.reshape(HEADS, KEY_DIM)
    queries = query_proj.astype(jnp.float32).reshape(seq_total, PROPOSALS, HEADS, KEY_DIM) * KEY_DIM ** (-0.5)
    forget = forget_of(forget_proj.reshape(seq_total, PROPOSALS, HEADS, KEY_DIM), bounds)
    new_values = value_proj.astype(jnp.float32).reshape(seq_total, PROPOSALS, HEADS, VAL_DIM)
    old_forget = forget_of(prev_forget.reshape(seq_total, PROPOSALS, HEADS, KEY_DIM), bounds)
    old_values = prev_value.astype(jnp.float32).reshape(seq_total, PROPOSALS, HEADS, VAL_DIM)
    taken, outputs = lax.map(lambda packed: recur_one(*packed), (state, old_forget, old_values, accepted, queries, forget, new_values))
    head_out = finish(outputs, head_gain, gate_proj)
    mixed = jnp.dot(head_out, w_out, preferred_element_type=jnp.float32).astype(jnp.bfloat16)
    return (mixed, taken)
```

```python
import jax
import jax.numpy as jnp
from jax import lax
from jax.experimental import pallas as pl
from jax.experimental.pallas import tpu as pltpu
from jax.sharding import PartitionSpec as P

EPSILON = 1e-06
F32 = jnp.float32
BF16 = jnp.bfloat16
VMEM = pl.BlockSpec(memory_space=pltpu.VMEM)
SMEM = pl.BlockSpec(memory_space=pltpu.SMEM)


def forget_of(pre_act, bounds):
    return bounds + (1.0 - bounds) * jax.nn.sigmoid(pre_act)


def norm_kernel(where, tokens, gain, own, *rest, ring, inner, share):
    mine, scratch = rest[:-1], rest[-1]
    rows, width = tokens.shape
    step = 16
    block = own.shape[-1]
    part = rows // share

    def one(i, carry):
        at = pl.multiple_of(i * step, step)
        x = tokens[pl.ds(at, step), :].astype(F32)
        scale = lax.rsqrt(jnp.mean(x * x, axis=-1, keepdims=True) + EPSILON)
        scratch[pl.ds(at, step), :] = (x * scale * gain[...]).astype(BF16)
        return carry

    lax.fori_loop(0, rows // step, one, 0)
    group, member, lane = where[0], where[1], where[2]
    for back in range(ring):
        owner = lax.rem(group - back + ring, ring)
        for turn in range(inner):
            column = owner * inner + lax.rem(member + turn, inner)
            cols = pl.ds(pl.multiple_of(column * block, block), block)
            if back == 0:
                own[turn] = scratch[:, cols]
            else:
                here = pl.ds(pl.multiple_of(lane * part, part), part)
                mine[back - 1][turn] = scratch[here, cols]


def project_kernel(where, own, *rest, ring, inner, share):
    others = rest[: (ring - 1) * share]
    weights = rest[(ring - 1) * share : (ring - 1) * share + inner]
    outs, lhs = rest[(ring - 1) * share + inner : -1], rest[-1]
    rows, block = own.shape[1], own.shape[2]
    part = rows // share
    lane = where[2]
    for turn in range(inner):
        cols = slice(turn * block, (turn + 1) * block)
        lhs[0:rows, cols] = own[turn]
        for r in range(ring - 1):
            for other in range(share):
                at = (r + 1) * rows + jnp.bitwise_xor(lane, other) * part
                lhs[pl.ds(pl.multiple_of(at, part), part), cols] = others[r * share + other][turn]
    for r in range(ring):
        here = slice(r * rows, (r + 1) * rows)
        total = None
        for turn in range(inner):
            product = jnp.dot(
                lhs[here, turn * block : (turn + 1) * block],
                weights[turn][...],
                preferred_element_type=F32,
            )
            total = product if total is None else total + product
        outs[r][...] = total.astype(outs[r].dtype)


def position_of(shape, proposals):
    return lax.rem(lax.broadcasted_iota(jnp.int32, shape, 0), proposals)


def taken_kernel(state, forget, values, keep, bounds, taken, *, proposals):
    seqs, heads, keys, vals = state.shape
    rows = seqs * proposals
    position = position_of((rows, keys), proposals)
    kept = keep[...] > 0.5
    decays, weights = [], []
    for head in range(heads):
        cols = slice(head * keys, (head + 1) * keys)
        gate = forget_of(forget[:, cols].astype(F32), bounds[:, cols])
        decay = jnp.where(kept, gate, 1.0)
        after = jnp.ones_like(decay)
        for ahead in range(1, proposals):
            moved = pltpu.roll(decay, rows - ahead, axis=0)
            after = after * jnp.where(position < proposals - ahead, moved, 1.0)
        decays.append(decay * after)
        weights.append(jnp.where(kept, 1.0 - gate, 0.0) * after)
    decay_columns = [d.T for d in decays]
    weight_columns = [w.T for w in weights]
    for head in range(heads):
        new = values[:, head * vals : (head + 1) * vals].astype(F32)
        for seq in range(seqs):
            at = seq * proposals
            total = decay_columns[head][:, at : at + 1] * state[seq, head]
            for t in range(proposals):
                total = total + weight_columns[head][:, at + t : at + t + 1] * new[at + t : at + t + 1, :]
            taken[seq, head] = total


def recur_kernel(*refs, parts, proposals):
    q_parts, f_parts, v_parts = refs[:parts], refs[parts : 2 * parts], refs[2 * parts : 3 * parts]
    taken, bounds, gain, out = refs[3 * parts :]
    seqs, heads, keys, vals = taken.shape
    rows = seqs * proposals
    position = position_of((rows, keys), proposals)
    group = 4
    tile = group * proposals
    tile_seq = lax.broadcasted_iota(jnp.int32, (tile, keys), 0) // proposals

    def total_of(pieces, cols):
        total = pieces[0][:, cols].astype(F32)
        for piece in pieces[1:]:
            total = total + piece[:, cols].astype(F32)
        return total

    for head in range(heads):
        cols = slice(head * keys, (head + 1) * keys)
        query = total_of(q_parts, cols) * keys ** (-0.5)
        gate = forget_of(total_of(f_parts, cols), bounds[:, cols])
        value = total_of(v_parts, cols)
        key = 1.0 - gate
        through = query
        result = jnp.sum(query * key, axis=-1, keepdims=True) * value
        for lag in range(1, proposals):
            through = through * jnp.where(
                position >= lag, pltpu.roll(gate, lag - 1, axis=0) if lag > 1 else gate, 0.0
            )
            score = jnp.sum(through * pltpu.roll(key, lag, axis=0), axis=-1, keepdims=True)
            result = result + score * pltpu.roll(value, lag, axis=0)
        grown = gate
        for lag in range(1, proposals):
            grown = grown * jnp.where(position >= lag, pltpu.roll(gate, lag, axis=0), 1.0)
        reach = (query * grown).astype(BF16)
        pieces = []
        for at in range(0, seqs, group):
            part = reach[at * proposals : (at + group) * proposals, :]
            lhs = jnp.concatenate(
                [jnp.where(tile_seq == s, part, jnp.zeros_like(part)) for s in range(group)], axis=1
            )
            here = taken[at : at + group, head].astype(BF16).reshape(group * keys, vals)
            pieces.append(jnp.dot(lhs, here, preferred_element_type=F32))
        result = result + jnp.concatenate(pieces, axis=0)
        scale = lax.rsqrt(jnp.mean(result * result, axis=-1, keepdims=True) + EPSILON)
        out[:, cols] = result * scale * gain[:, cols]


def mix_kernel(where, *refs, lanes, blocks):
    heads, weights = refs[:lanes], refs[lanes : lanes + blocks]
    out, lhs = refs[lanes + blocks :]
    height = weights[0].shape[0]
    per = heads[0].shape[1] // height
    for other in range(lanes):
        lane = jnp.bitwise_xor(where[0], other)
        for k in range(per):
            lhs[lane * per + k] = heads[other][:, k * height : (k + 1) * height]
    total = None
    for j in range(blocks):
        product = jnp.dot(lhs[where[1 + j]], weights[j][...], preferred_element_type=F32)
        total = product if total is None else total + product
    out[...] = total.astype(out.dtype)


def on_device(
    tokens,
    norm_gain,
    w_query,
    w_forget,
    w_value,
    w_gate,
    lower_bound,
    head_gain,
    w_out,
    state,
    prev_forget,
    prev_value,
    accepted,
    *,
    kv,
    tp,
):
    seqs, heads, keys, vals = state.shape
    proposals = prev_forget.shape[1]
    rows = tokens.shape[0]
    width = heads * keys
    inner = 2 if kv % 2 == 0 else 1
    ring = kv // inner
    share = 2 if tp % 2 == 0 else 1
    me = lax.axis_index("kv")
    lane = lax.axis_index("tp")
    group, member = me // inner, me % inner
    where = jnp.stack([group, member, lane % share]).astype(jnp.int32)

    def along(shift):
        return [((g * inner + m), ((g + shift) % ring) * inner + m) for g in range(ring) for m in range(inner)]

    def line(shift):
        return [
            (g * inner + m, (g + shift) * inner + m)
            for g in range(ring)
            for m in range(inner)
            if 0 <= g + shift < ring
        ]

    def around(turn):
        return [(g * inner + (m + turn) % inner, g * inner + m) for g in range(ring) for m in range(inner)]

    def swap(bit):
        return [(t, t ^ bit) for t in range(tp)]

    sets = []
    for weight in (w_forget, w_value, w_query, w_gate):
        sets.append([weight] + [lax.ppermute(weight, "kv", around(t)) for t in range(1, inner)])

    block = w_query.shape[0]
    part = rows // share
    shapes = [jax.ShapeDtypeStruct((inner, rows, block), BF16)]
    shapes += [jax.ShapeDtypeStruct((inner, part, block), BF16)] * (ring - 1)
    normed = pl.pallas_call(
        lambda *refs: norm_kernel(*refs, ring=ring, inner=inner, share=share),
        out_shape=shapes,
        in_specs=[SMEM, VMEM, VMEM],
        out_specs=[VMEM] * ring,
        scratch_shapes=[pltpu.VMEM(tokens.shape, BF16)],
        name="norm",
    )(where, tokens, norm_gain.reshape(1, -1))
    own, mine = normed[0], normed[1:]
    others = []
    for back in range(1, ring):
        got = lax.ppermute(mine[back - 1], "kv", along(-back))
        others.append(got)
        for bit in range(1, share):
            others.append(lax.ppermute(got, "tp", swap(bit)))

    position = jnp.arange(proposals)
    keep = jnp.broadcast_to(
        (position[None, :] < accepted[:, None]).astype(F32).reshape(-1, 1), (seqs * proposals, keys)
    )
    bounds = lower_bound.reshape(1, width)
    some = 8 if seqs % 8 == 0 else seqs
    some_rows = some * proposals
    state_spec = pl.BlockSpec((some, heads, keys, vals), lambda i: (i, 0, 0, 0))
    row_spec = pl.BlockSpec((some_rows, width), lambda i: (i, 0))
    one_spec = pl.BlockSpec((1, width), lambda i: (0, 0))
    taken = pl.pallas_call(
        lambda *refs: taken_kernel(*refs, proposals=proposals),
        out_shape=jax.ShapeDtypeStruct(state.shape, F32),
        grid=(seqs // some,),
        in_specs=[
            state_spec,
            row_spec,
            row_spec,
            pl.BlockSpec((some_rows, keys), lambda i: (i, 0)),
            one_spec,
        ],
        out_specs=state_spec,
        name="taken",
    )(state, prev_forget.reshape(rows, width), prev_value.reshape(rows, width), keep, bounds)

    def summed(weights):
        products = pl.pallas_call(
            lambda *refs: project_kernel(*refs, ring=ring, inner=inner, share=share),
            out_shape=[jax.ShapeDtypeStruct((rows, width), F32 if r == 0 else BF16) for r in range(ring)],
            in_specs=[SMEM] + [VMEM] * (1 + len(others) + inner),
            out_specs=[VMEM] * ring,
            scratch_shapes=[pltpu.VMEM((ring * rows, inner * block), BF16)],
            name="project",
        )(where, own, *others, *weights)
        if ring == 1:
            return [products[0]]
        up = down = None
        for step in range(1, ring):
            up_part, down_part = products[ring - step], products[step]
            if up is not None:
                up_part = (up_part.astype(F32) + up.astype(F32)).astype(BF16)
                down_part = (down_part.astype(F32) + down.astype(F32)).astype(BF16)
            span = [(s, d) for s, d in line(1) if s // inner < step]
            up = lax.ppermute(up_part, "kv", span)
            span = [(s, d) for s, d in line(-1) if s // inner >= ring - step]
            down = lax.ppermute(down_part, "kv", span)
        return [products[0], up, down]

    forget_parts, value_parts, query_parts, gate_parts = [summed(weights) for weights in sets]

    blocks, places = [], []
    for ahead in range(ring):
        piece = w_out if ahead == 0 else lax.ppermute(w_out, "kv", along(-ahead))
        for turn in range(inner):
            blocks.append(piece if turn == 0 else lax.ppermute(piece, "kv", around(turn)))
            places.append(((group + ahead) % ring) * inner + (member + turn) % inner)

    parts = len(query_parts)
    scaled = pl.pallas_call(
        lambda *refs: recur_kernel(*refs, parts=parts, proposals=proposals),
        out_shape=jax.ShapeDtypeStruct((rows, width), F32),
        grid=(seqs // some,),
        in_specs=[row_spec] * (3 * parts) + [state_spec, one_spec, one_spec],
        out_specs=row_spec,
        name="recur",
    )(*query_parts, *forget_parts, *value_parts, taken, bounds, head_gain.reshape(1, width))
    gate = sum(piece.astype(F32) for piece in gate_parts)
    head_out = (scaled * jax.nn.silu(gate)).astype(BF16)

    gathered = [head_out]
    bit = 1
    while bit < tp:
        gathered += [lax.ppermute(piece, "tp", swap(bit)) for piece in gathered]
        bit *= 2
    table = jnp.stack([lane] + places).astype(jnp.int32)
    height = w_out.shape[0]
    mixed = pl.pallas_call(
        lambda *refs: mix_kernel(*refs, lanes=tp, blocks=kv),
        out_shape=jax.ShapeDtypeStruct((rows, w_out.shape[1]), BF16),
        in_specs=[SMEM] + [VMEM] * (tp + kv),
        out_specs=VMEM,
        scratch_shapes=[pltpu.VMEM((kv, rows, height), BF16)],
        name="mix",
    )(table, *gathered, *blocks)
    return (mixed, taken)


def solution(mesh):
    kv, tp = mesh.shape["kv"], mesh.shape["tp"]
    return jax.shard_map(
        lambda *args: on_device(*args, kv=kv, tp=tp),
        mesh=mesh,
        in_specs=(
            P("kv", None),
            P(),
            P("kv", "tp"),
            P("kv", "tp"),
            P("kv", "tp"),
            P("kv", "tp"),
            P("tp"),
            P("tp"),
            P("kv", "tp"),
            P("kv", "tp", None, None),
            P("kv", None, "tp"),
            P("kv", None, "tp"),
            P("kv"),
        ),
        out_specs=(P("kv", "tp"), P("kv", "tp", None, None)),
        check_vma=False,
    )
```

```python
import jax
import jax.numpy as jnp
import numpy as np
from jax import lax
from jax.experimental import pallas as pl
from jax.experimental.pallas import tpu as pltpu
from jax.sharding import PartitionSpec as P


EPSILON = 1e-06
F32 = jnp.float32
BF16 = jnp.bfloat16
VMEM = pl.BlockSpec(memory_space=pltpu.VMEM)
SMEM = pl.BlockSpec(memory_space=pltpu.SMEM)


def forget_of(pre_act, bounds):
    return bounds + (1.0 - bounds) * jax.nn.sigmoid(pre_act)


def norm_kernel(tokens, gain, own, *rest, ring, inner, share):
    mine, scratch = rest[:-1], rest[-1]
    rows, width = tokens.shape
    step = 16
    block = own.shape[-1]
    part = rows // share
    chunk = min(width, 512)

    def one(i, carry):
        here = pl.ds(pl.multiple_of(i * step, step), step)
        total = jnp.zeros((step, 128), F32)
        for at in range(0, width, chunk):
            x = tokens[here, at : at + chunk].astype(F32)
            x = x * x
            for k in range(0, chunk, 128):
                total = total + x[:, k : k + 128]
        scale = lax.rsqrt(jnp.sum(total, axis=-1, keepdims=True) / width + EPSILON)
        for at in range(0, width, chunk):
            x = tokens[here, at : at + chunk].astype(F32)
            scratch[here, at : at + chunk] = (x * scale * gain[:, at : at + chunk]).astype(BF16)
        return carry

    lax.fori_loop(0, rows // step, one, 0)
    me, lane = lax.axis_index("kv"), lax.axis_index("tp")
    group, member = lax.div(me, inner), lax.rem(me, inner)
    here = pl.ds(pl.multiple_of(lax.rem(lane, share) * part, part), part)
    for r in range(ring):
        owner = jnp.bitwise_xor(group, r)
        for turn in range(inner):
            column = owner * inner + lax.rem(member + turn, inner)
            cols = pl.ds(pl.multiple_of(column * block, block), block)
            if r == 0:
                own[turn] = scratch[:, cols]
            else:
                mine[r - 1][turn] = scratch[here, cols]


def project_kernel(own, *rest, ring, inner, share):
    others = rest[: (ring - 1) * share]
    weights = rest[(ring - 1) * share : (ring - 1) * share + inner]
    outs, lhs = rest[(ring - 1) * share + inner : -1], rest[-1]
    rows, block = own.shape[1], own.shape[2]
    part = rows // share
    lane = lax.rem(lax.axis_index("tp"), share)
    for turn in range(inner):
        cols = slice(turn * block, (turn + 1) * block)
        lhs[0:rows, cols] = own[turn]
        for r in range(ring - 1):
            for other in range(share):
                at = (r + 1) * rows + jnp.bitwise_xor(lane, other) * part
                lhs[pl.ds(pl.multiple_of(at, part), part), cols] = others[r * share + other][turn]
    level = 0
    for r in range(ring):
        here = slice(r * rows, (r + 1) * rows)
        total = None
        for turn in range(inner):
            product = jnp.dot(
                lhs[here, turn * block : (turn + 1) * block],
                weights[turn][...],
                preferred_element_type=F32,
            )
            total = product if total is None else total + product
        if r == 0:
            outs[0][...] = total
        else:
            level = r.bit_length()
            outs[level][r - (1 << (level - 1))] = total.astype(BF16)


def position_of(shape, proposals):
    return lax.rem(lax.broadcasted_iota(jnp.int32, shape, 0), proposals)


def taken_kernel(accepted, state, forget, values, bounds, taken, rounded, *, proposals):
    seqs, heads, keys, vals = state.shape
    rows = seqs * proposals
    first = pl.program_id(0) * seqs
    position = position_of((rows, keys), proposals)
    owner = lax.broadcasted_iota(jnp.int32, (rows, keys), 0) // proposals
    count = jnp.zeros((rows, keys), jnp.int32)
    for seq in range(seqs):
        count = jnp.where(owner == seq, accepted[first + seq], count)
    kept = position < count
    for head in range(heads):
        cols = slice(head * keys, (head + 1) * keys)
        gate = forget_of(forget[:, cols].astype(F32), bounds[:, cols])
        decay = jnp.where(kept, gate, 1.0)
        after = jnp.ones_like(decay)
        for ahead in range(1, proposals):
            moved = pltpu.roll(decay, rows - ahead, axis=0)
            after = after * jnp.where(position < proposals - ahead, moved, 1.0)
        decay_columns = (decay * after).T
        weight = (jnp.where(kept, 1.0 - gate, 0.0) * after).T
        high = weight.astype(BF16)
        low = (weight - high.astype(F32)).astype(BF16)
        new = values[:, head * vals : (head + 1) * vals]
        spread = jnp.concatenate(
            [jnp.where(owner == seq, new, jnp.zeros_like(new)) for seq in range(seqs)], axis=1
        )
        added = jnp.dot(
            jnp.concatenate([high, low], axis=1),
            jnp.concatenate([spread, spread], axis=0),
            preferred_element_type=F32,
        )
        for seq in range(seqs):
            at = seq * proposals
            total = (
                decay_columns[:, at : at + 1] * state[seq, head] + added[:, seq * vals : (seq + 1) * vals]
            )
            taken[seq, head] = total
            rounded[seq, head] = total.astype(BF16)


def recur_kernel(*refs, parts, proposals):
    q_parts, f_parts, v_parts = refs[:parts], refs[parts : 2 * parts], refs[2 * parts : 3 * parts]
    taken, bounds, gain, out = refs[3 * parts :]
    seqs, heads, keys, vals = taken.shape
    rows = seqs * proposals
    position = position_of((rows, keys), proposals)
    group = 4
    tile = group * proposals
    tile_seq = lax.broadcasted_iota(jnp.int32, (tile, keys), 0) // proposals

    def total_of(pieces, cols):
        total = pieces[0][:, cols]
        for piece in pieces[1:]:
            total = total + piece[0, :, cols].astype(F32)
        return total

    for head in range(heads):
        cols = slice(head * keys, (head + 1) * keys)
        query = total_of(q_parts, cols) * keys ** (-0.5)
        gate = forget_of(total_of(f_parts, cols), bounds[:, cols])
        value = total_of(v_parts, cols)
        key = 1.0 - gate
        through = query
        result = jnp.sum(query * key, axis=-1, keepdims=True) * value
        for lag in range(1, proposals):
            through = through * jnp.where(
                position >= lag, pltpu.roll(gate, lag - 1, axis=0) if lag > 1 else gate, 0.0
            )
            score = jnp.sum(through * pltpu.roll(key, lag, axis=0), axis=-1, keepdims=True)
            result = result + score * pltpu.roll(value, lag, axis=0)
        grown = gate
        for lag in range(1, proposals):
            grown = grown * jnp.where(position >= lag, pltpu.roll(gate, lag, axis=0), 1.0)
        reach = (query * grown).astype(BF16)
        pieces = []
        for at in range(0, seqs, group):
            part = reach[at * proposals : (at + group) * proposals, :]
            lhs = jnp.concatenate(
                [jnp.where(tile_seq == s, part, jnp.zeros_like(part)) for s in range(group)], axis=1
            )
            here = taken[at : at + group, head].reshape(group * keys, vals)
            pieces.append(jnp.dot(lhs, here, preferred_element_type=F32))
        result = result + jnp.concatenate(pieces, axis=0)
        scale = lax.rsqrt(jnp.mean(result * result, axis=-1, keepdims=True) + EPSILON)
        out[:, cols] = result * scale * gain[:, cols]


def mix_kernel(order, *refs, lanes, ids, inner):
    heads, weights = refs[:lanes], refs[lanes:-2]
    out, lhs = refs[-2:]
    height = weights[0].shape[1]
    per = heads[0].shape[1] // height
    mine = lax.axis_index("tp")
    me = lax.axis_index("kv")
    group, member = lax.div(me, inner), lax.rem(me, inner)
    for head, other in zip(heads, ids):
        lane = jnp.bitwise_xor(mine, other)
        for k in range(per):
            lhs[lane * per + k] = head[:, k * height : (k + 1) * height]
    total = None
    slot = 0
    for at in range(0, len(weights), inner):
        for k in range(weights[at].shape[0]):
            for turn in range(inner):
                place = order[group, slot] * inner + lax.rem(member + turn, inner)
                product = jnp.dot(lhs[place], weights[at + turn][k], preferred_element_type=F32)
                total = product if total is None else total + product
            slot += 1
    out[...] = total.astype(out.dtype)


def on_device(
    tokens,
    norm_gain,
    w_query,
    w_forget,
    w_value,
    w_gate,
    lower_bound,
    head_gain,
    w_out,
    state,
    prev_forget,
    prev_value,
    accepted,
    *,
    kv,
    tp,
):
    seqs, heads, keys, vals = state.shape
    proposals = prev_forget.shape[1]
    rows = tokens.shape[0]
    width = heads * keys
    inner, ring, share = cut_of(kv, tp)

    def groups(pairs):
        return [(a * inner + m, b * inner + m) for a, b in pairs for m in range(inner)]

    def around(turn):
        return [(g * inner + (m + turn) % inner, g * inner + m) for g in range(ring) for m in range(inner)]

    def mirrored(size, start, stop):
        pairs = []
        for base in range(0, ring, 2 * size):
            last = base + 2 * size - 1
            pairs += [(base + start, base + stop), (last - start, last - stop)]
        return groups(pairs)

    def swap(value, bit):
        return lax.ppermute(value, "tp", [(t, t ^ bit) for t in range(tp)])

    sets = []
    for weight in (w_forget, w_value, w_query, w_gate):
        sets.append([weight] + [lax.ppermute(weight, "kv", around(t)) for t in range(1, inner)])

    block = w_query.shape[0]
    part = rows // share
    shapes = [jax.ShapeDtypeStruct((inner, rows, block), BF16)]
    shapes += [jax.ShapeDtypeStruct((inner, part, block), BF16)] * (ring - 1)
    normed = pl.pallas_call(
        lambda *refs: norm_kernel(*refs, ring=ring, inner=inner, share=share),
        out_shape=shapes,
        in_specs=[VMEM, VMEM],
        out_specs=[VMEM] * ring,
        scratch_shapes=[pltpu.VMEM(tokens.shape, BF16)],
        name="norm",
    )(tokens, norm_gain.reshape(1, -1))
    own, mine = normed[0], normed[1:]
    others = []
    for r in range(1, ring):
        got = lax.ppermute(mine[r - 1], "kv", groups([(g, g ^ r) for g in range(ring)]))
        others.append(got)
        for bit in range(1, share):
            others.append(swap(got, bit))

    bounds = lower_bound.reshape(1, width)
    some = 8 if seqs % 8 == 0 else seqs
    some_rows = some * proposals
    state_spec = pl.BlockSpec((some, heads, keys, vals), lambda i: (i, 0, 0, 0))
    row_spec = pl.BlockSpec((some_rows, width), lambda i: (i, 0))
    one_spec = pl.BlockSpec((1, width), lambda i: (0, 0))
    taken, rounded = pl.pallas_call(
        lambda *refs: taken_kernel(*refs, proposals=proposals),
        out_shape=[jax.ShapeDtypeStruct(state.shape, F32), jax.ShapeDtypeStruct(state.shape, BF16)],
        grid=(seqs // some,),
        in_specs=[SMEM, state_spec, row_spec, row_spec, one_spec],
        out_specs=[state_spec, state_spec],
        name="taken",
    )(accepted, state, prev_forget.reshape(rows, width), prev_value.reshape(rows, width), bounds)

    def added(a, b):
        return (a.astype(F32) + b.astype(F32)).astype(BF16)

    def summed(weights):
        levels = [1 << k for k in range((ring - 1).bit_length())]
        shapes = [jax.ShapeDtypeStruct((rows, width), F32)]
        shapes += [jax.ShapeDtypeStruct((size, rows, width), BF16) for size in levels]
        products = pl.pallas_call(
            lambda *refs: project_kernel(*refs, ring=ring, inner=inner, share=share),
            out_shape=shapes,
            in_specs=[VMEM] * (1 + len(others) + inner),
            out_specs=[VMEM] * len(shapes),
            scratch_shapes=[pltpu.VMEM((ring * rows, inner * block), BF16)],
            name="project",
        )(own, *others, *weights)
        pieces = [(products[0], 0)]
        held = {size: products[1 + k] for k, size in enumerate(levels)}
        for size in reversed(levels):
            out = held[size]
            for hop in range(1, size):
                got = lax.ppermute(out, "kv", mirrored(size, hop - 1, hop))
                turn = (hop - 1) ^ hop
                out = added(out, jnp.stack([got[k ^ turn] for k in range(size)]))
            got = lax.ppermute(out, "kv", mirrored(size, size - 1, size))
            pieces.append((got, size - 1))
            for lower in levels:
                if lower < size:
                    kept = [got[(j ^ (2 * size - 1)) - size] for j in range(lower, 2 * lower)]
                    held[lower] = added(held[lower], jnp.stack(kept))
        return pieces

    forget_parts, value_parts, query_parts, gate_parts = [summed(weights) for weights in sets]

    blocks = []
    cur = w_out[None]
    size, step = 1, 0
    while size < ring:
        got = lax.ppermute(cur, "kv", mirrored(size, size - 1, size))
        step += 1
        total = got
        for hop in range(1, size):
            got = lax.ppermute(got, "kv", mirrored(size, size - hop, size - hop - 1))
            step += 1
            total = total + got
        if size == 1:
            cur = jnp.concatenate([cur, total])
            fresh = cur
        else:
            fresh = total
            if 2 * size < ring:
                cur = jnp.concatenate([cur, total])
        blocks.append(fresh)
        size *= 2
    if ring == 1:
        blocks = [cur]
    weights = []
    for fresh in blocks:
        weights += [fresh] + [lax.ppermute(fresh, "kv", around(t)) for t in range(1, inner)]

    def specs_of(pieces):
        specs, arrays = [], []
        for array, index in pieces:
            arrays.append(array)
            if array.ndim == 2:
                specs.append(row_spec)
            else:
                specs.append(pl.BlockSpec((1, some_rows, width), lambda i, index=index: (index, i, 0)))
        return specs, arrays

    specs, arrays = [], []
    for pieces in (query_parts, forget_parts, value_parts):
        more_specs, more = specs_of(pieces)
        specs += more_specs
        arrays += more
    parts = len(query_parts)
    scaled = pl.pallas_call(
        lambda *refs: recur_kernel(*refs, parts=parts, proposals=proposals),
        out_shape=jax.ShapeDtypeStruct((rows, width), F32),
        grid=(seqs // some,),
        in_specs=specs + [state_spec, one_spec, one_spec],
        out_specs=row_spec,
        name="recur",
    )(*arrays, rounded, bounds, head_gain.reshape(1, width))
    gate = gate_parts[0][0]
    for array, index in gate_parts[1:]:
        gate = gate + array[index].astype(F32)
    head_out = (scaled * jax.nn.silu(gate)).astype(BF16)

    gathered, ids = [head_out], [0]
    bit = tp // 2
    while bit:
        gathered += [swap(piece, bit) for piece in gathered]
        ids += [i ^ bit for i in ids]
        bit //= 2
    table = jnp.asarray(order_of(ring), jnp.int32)
    height = w_out.shape[0]
    mixed = pl.pallas_call(
        lambda *refs: mix_kernel(*refs, lanes=tp, ids=ids, inner=inner),
        out_shape=jax.ShapeDtypeStruct((rows, w_out.shape[1]), BF16),
        in_specs=[SMEM] + [VMEM] * (tp + len(weights)),
        out_specs=VMEM,
        scratch_shapes=[pltpu.VMEM((kv, rows, height), BF16)],
        name="mix",
    )(table, *gathered, *weights)
    return (mixed, taken)


def cut_of(kv, tp):
    inner = 2 if kv % 2 == 0 else 1
    return inner, kv // inner, 2 if tp % 2 == 0 else 1


def order_of(ring):
    order = [[g] for g in range(ring)]
    size = 1
    while size < ring:
        order = [
            order[g] + order[(g // (2 * size)) * 2 * size + (size if g % (2 * size) < size else size - 1)]
            for g in range(ring)
        ]
        size *= 2
    return np.array(order, np.int32)


def solution(mesh):
    kv, tp = mesh.shape["kv"], mesh.shape["tp"]

    def body(*args):
        return on_device(*args, kv=kv, tp=tp)

    return jax.shard_map(
        body,
        mesh=mesh,
        in_specs=(
            P("kv", None),
            P(),
            P("kv", "tp"),
            P("kv", "tp"),
            P("kv", "tp"),
            P("kv", "tp"),
            P("tp"),
            P("tp"),
            P("kv", "tp"),
            P("kv", "tp", None, None),
            P("kv", None, "tp"),
            P("kv", None, "tp"),
            P("kv"),
        ),
        out_specs=(P("kv", "tp"), P("kv", "tp", None, None)),
        check_vma=False,
    )
```

```python
import jax
import jax.numpy as jnp
import numpy as np
from jax import lax
from jax.experimental import pallas as pl
from jax.experimental.pallas import tpu as pltpu
from jax.sharding import PartitionSpec as P


EPSILON = 1e-06
F32 = jnp.float32
BF16 = jnp.bfloat16
VMEM = pl.BlockSpec(memory_space=pltpu.VMEM)
SMEM = pl.BlockSpec(memory_space=pltpu.SMEM)
HBM = pl.BlockSpec(memory_space=pltpu.MemorySpace.HBM)


def room(mib):
    return pltpu.CompilerParams(vmem_limit_bytes=mib << 20)


def forget_of(pre_act, bounds):
    return bounds + (1.0 - bounds) * jax.nn.sigmoid(pre_act)


def norm_kernel(tokens, gain, *refs, ring, inner, share, heads):
    weights, own, mine = refs[:4], refs[4], refs[5 : 4 + ring]
    pieces, (scratch, sems) = refs[4 + ring : -2], refs[-2:]
    keys = weights[0].shape[1] // heads
    copies = [
        pltpu.make_async_copy(
            weights[k].at[:, pl.ds(head * keys, keys)],
            pieces[head].at[:, pl.ds(k * keys, keys)],
            sems.at[head * 4 + k],
        )
        for head in range(heads)
        for k in range(4)
    ]
    for copy in copies:
        copy.start()
    rows, width = tokens.shape
    step = 16
    block = own.shape[-1]
    part = rows // share
    chunk = min(width, 512)

    def one(i, carry):
        here = pl.ds(pl.multiple_of(i * step, step), step)
        total = jnp.zeros((step, 128), F32)
        for at in range(0, width, chunk):
            x = tokens[here, at : at + chunk].astype(F32)
            x = x * x
            for k in range(0, chunk, 128):
                total = total + x[:, k : k + 128]
        scale = lax.rsqrt(jnp.sum(total, axis=-1, keepdims=True) / width + EPSILON)
        for at in range(0, width, chunk):
            x = tokens[here, at : at + chunk].astype(F32)
            scratch[here, at : at + chunk] = (x * scale * gain[:, at : at + chunk]).astype(BF16)
        return carry

    lax.fori_loop(0, rows // step, one, 0, unroll=4)
    me, lane = lax.axis_index("kv"), lax.axis_index("tp")
    group, member = lax.div(me, inner), lax.rem(me, inner)
    here = pl.ds(pl.multiple_of(lax.rem(lane, share) * part, part), part)
    for r in range(ring):
        owner = jnp.bitwise_xor(group, r)
        for turn in range(inner):
            column = owner * inner + lax.rem(member + turn, inner)
            cols = pl.ds(pl.multiple_of(column * block, block), block)
            if r == 0:
                own[turn] = scratch[:, cols]
            else:
                mine[r - 1][turn] = scratch[here, cols]
    for copy in copies:
        copy.wait()


def project_kernel(*refs, ring, inner, share, fresh):
    if fresh:
        own, others = refs[0], refs[1 : 1 + (ring - 1) * share]
        weights = refs[1 + (ring - 1) * share :][:inner]
        outs, lhs, stack = refs[1 + (ring - 1) * share + inner : -2], refs[-2], refs[-1]
        rows, block = own.shape[1], own.shape[2]
        part = rows // share
        lane = lax.rem(lax.axis_index("tp"), share)
        for turn in range(inner):
            cols = slice(turn * block, (turn + 1) * block)
            lhs[0:rows, cols] = own[turn]
            for r in range(ring - 1):
                for other in range(share):
                    at = (r + 1) * rows + jnp.bitwise_xor(lane, other) * part
                    lhs[pl.ds(pl.multiple_of(at, part), part), cols] = others[r * share + other][turn]
    else:
        lhs, weights = refs[0], refs[1 : 1 + inner]
        outs, stack = refs[1 + inner : -1], refs[-1]
        block = weights[0].shape[0]
        rows = lhs.shape[0] // ring
    group = lax.div(lax.axis_index("kv"), inner)
    for turn in range(inner):
        stack[turn * block : (turn + 1) * block, :] = weights[turn][...]
    for level in reversed(range(len(outs))):
        size = 1 << max(level - 1, 0)
        start = size if level else 0
        total = jnp.dot(
            lhs[start * rows : (start + size) * rows, :], stack[...], preferred_element_type=F32
        )
        if level:
            for k in range(size):
                at = jnp.bitwise_xor(lax.rem(group, size), k)
                outs[level][at] = total[k * rows : (k + 1) * rows].astype(BF16)
        else:
            outs[0][...] = total


def position_of(shape, proposals):
    return lax.rem(lax.broadcasted_iota(jnp.int32, shape, 0), proposals)


def taken_kernel(accepted, state, forget, values, bounds, taken, held, come, gone, *, proposals, seqs):
    count, heads, keys, vals = state.shape
    steps = count // seqs
    rows = seqs * proposals
    position = position_of((rows, keys), proposals)
    owner = lax.broadcasted_iota(jnp.int32, (rows, keys), 0) // proposals

    def copy_in(i):
        here = pl.ds(i * seqs, seqs)
        return pltpu.make_async_copy(state.at[here], held.at[here], come.at[i])

    def copy_out(i):
        here = pl.ds(i * seqs, seqs)
        return pltpu.make_async_copy(held.at[here], taken.at[here], gone.at[i])

    for i in range(steps):
        copy_in(i).start()

    def one(i, carry):
        first = i * seqs
        old = jnp.concatenate([forget[first + seq].astype(F32) for seq in range(seqs)], axis=0)
        new = jnp.concatenate([values[first + seq].astype(F32) for seq in range(seqs)], axis=0).astype(BF16)
        taking = jnp.zeros((rows, keys), jnp.int32)
        for seq in range(seqs):
            taking = jnp.where(owner == seq, accepted[first + seq], taking)
        kept = position < taking
        decays, addeds = [], []
        for head in range(heads):
            cols = slice(head * keys, (head + 1) * keys)
            gate = forget_of(old[:, cols], bounds[:, cols])
            decay = jnp.where(kept, gate, 1.0)
            after = jnp.ones_like(decay)
            for ahead in range(1, proposals):
                moved = pltpu.roll(decay, rows - ahead, axis=0)
                after = after * jnp.where(position < proposals - ahead, moved, 1.0)
            decays.append((decay * after).T)
            weight = (jnp.where(kept, 1.0 - gate, 0.0) * after).T
            high = weight.astype(BF16)
            low = (weight - high.astype(F32)).astype(BF16)
            value = new[:, head * vals : (head + 1) * vals]
            spread = jnp.concatenate(
                [jnp.where(owner == seq, value, jnp.zeros_like(value)) for seq in range(seqs)], axis=1
            )
            addeds.append(
                jnp.dot(
                    jnp.concatenate([high, low], axis=1),
                    jnp.concatenate([spread, spread], axis=0),
                    preferred_element_type=F32,
                )
            )
        copy_in(i).wait()
        for head in range(heads):
            for seq in range(seqs):
                at = seq * proposals
                held[first + seq, head] = (
                    decays[head][:, at : at + 1] * held[first + seq, head]
                    + addeds[head][:, seq * vals : (seq + 1) * vals]
                )
        copy_out(i).start()
        return carry

    lax.fori_loop(0, steps, one, 0)
    for i in range(steps):
        copy_out(i).wait()


def recur_kernel(*refs, parts, heads, first, proposals, inner):
    pieces = refs[: parts * heads]
    taken, bounds, gain, out = refs[parts * heads :]
    where = lax.div(lax.axis_index("kv"), inner)
    seqs, _, keys, vals = taken.shape
    rows = seqs * proposals
    position = position_of((rows, keys), proposals)
    group = 4
    tile = group * proposals
    tile_seq = lax.broadcasted_iota(jnp.int32, (tile, keys), 0) // proposals

    def total_of(head, k):
        cols = slice(k * keys, (k + 1) * keys)
        total = pieces[head * parts][:, cols]
        for piece in pieces[head * parts + 1 : (head + 1) * parts]:
            total = total + piece[lax.rem(where, piece.shape[0]), :, cols].astype(F32)
        return total

    for head in range(heads):
        cols = slice((first + head) * keys, (first + head + 1) * keys)
        gate = forget_of(total_of(head, 0), bounds[:, cols])
        value = total_of(head, 1)
        query = total_of(head, 2) * keys ** (-0.5)
        key = 1.0 - gate
        through = query
        result = jnp.sum(query * key, axis=-1, keepdims=True) * value
        grown = gate
        before = gate
        for lag in range(1, proposals):
            inside = position >= lag
            through = through * jnp.where(inside, before, 0.0)
            score = jnp.sum(through * pltpu.roll(key, lag, axis=0), axis=-1, keepdims=True)
            result = result + score * pltpu.roll(value, lag, axis=0)
            before = pltpu.roll(gate, lag, axis=0)
            grown = grown * jnp.where(inside, before, 1.0)
        reach = (query * grown).astype(BF16)
        met = []
        for at in range(0, seqs, group):
            part = reach[at * proposals : (at + group) * proposals, :]
            lhs = jnp.concatenate(
                [jnp.where(tile_seq == s, part, jnp.zeros_like(part)) for s in range(group)], axis=1
            )
            here = taken[at : at + group, head].astype(BF16).reshape(group * keys, vals)
            met.append(jnp.dot(lhs, here, preferred_element_type=F32))
        result = result + jnp.concatenate(met, axis=0)
        scale = lax.rsqrt(jnp.mean(result * result, axis=-1, keepdims=True) + EPSILON)
        result = result * scale * gain[:, cols] * jax.nn.silu(total_of(head, 3))
        out[:, head * keys : (head + 1) * keys] = result.astype(BF16)


def mix_kernel(order, *refs, lanes, ids, runs, inner, keys):
    heads, weights = refs[: lanes * len(runs)], refs[lanes * len(runs) : -2]
    out, lhs = refs[-2:]
    height = weights[0].shape[1]
    per = height // keys
    count = sum(len(run) for run in runs)
    mine = lax.axis_index("tp")
    me = lax.axis_index("kv")
    group, member = lax.div(me, inner), lax.rem(me, inner)
    for at, run in enumerate(runs):
        for k, other in enumerate(ids):
            lane = jnp.bitwise_xor(mine, other)
            for j, head in enumerate(run):
                where = lane * (count // per) + head // per
                cols = slice(head % per * keys, (head % per + 1) * keys)
                lhs[where, :, cols] = heads[at * lanes + k][:, j * keys : (j + 1) * keys]
    chunk = min(out.shape[1], 256)
    for n in range(0, out.shape[1], chunk):
        total = None
        slot = 0
        for at in range(0, len(weights), inner):
            for k in range(weights[at].shape[0]):
                for turn in range(inner):
                    place = order[group, slot] * inner + lax.rem(member + turn, inner)
                    product = jnp.dot(
                        lhs[place], weights[at + turn][k, :, n : n + chunk], preferred_element_type=F32
                    )
                    total = product if total is None else total + product
                slot += 1
        out[:, n : n + chunk] = total.astype(out.dtype)


def on_device(
    tokens,
    norm_gain,
    w_query,
    w_forget,
    w_value,
    w_gate,
    lower_bound,
    head_gain,
    w_out,
    state,
    prev_forget,
    prev_value,
    accepted,
    *,
    kv,
    tp,
):
    seqs, heads, keys, vals = state.shape
    proposals = prev_forget.shape[1]
    rows = tokens.shape[0]
    width = heads * keys
    inner, ring, share = cut_of(kv, tp)

    group = lax.axis_index("kv") // inner

    def groups(pairs):
        return [(a * inner + m, b * inner + m) for a, b in pairs for m in range(inner)]

    def around(turn):
        return [(g * inner + (m + turn) % inner, g * inner + m) for g in range(ring) for m in range(inner)]

    def mirrored(size, start, stop):
        pairs = []
        for base in range(0, ring, 2 * size):
            last = base + 2 * size - 1
            pairs += [(base + start, base + stop), (last - start, last - stop)]
        return groups(pairs)

    def swap(value, bit):
        return lax.ppermute(value, "tp", [(t, t ^ bit) for t in range(tp)])

    block = w_query.shape[0]
    part = rows // share
    shapes = [jax.ShapeDtypeStruct((inner, rows, block), BF16)]
    shapes += [jax.ShapeDtypeStruct((inner, part, block), BF16)] * (ring - 1)
    shapes += [jax.ShapeDtypeStruct((block, 4 * keys), BF16)] * heads
    normed = pl.pallas_call(
        lambda *refs: norm_kernel(*refs, ring=ring, inner=inner, share=share, heads=heads),
        out_shape=shapes,
        in_specs=[VMEM, VMEM] + [HBM] * 4,
        out_specs=[VMEM] * len(shapes),
        scratch_shapes=[pltpu.VMEM(tokens.shape, BF16), pltpu.SemaphoreType.DMA((4 * heads,))],
        compiler_params=room(60),
        name="norm",
    )(tokens, norm_gain.reshape(1, -1), w_forget, w_value, w_query, w_gate)
    own, mine = normed[0], normed[1:ring]
    sets = []
    for weight in normed[ring:]:
        sets.append([weight] + [lax.ppermute(weight, "kv", around(t)) for t in range(1, inner)])
    others = []
    for r in range(1, ring):
        got = lax.ppermute(mine[r - 1], "kv", groups([(g, g ^ r) for g in range(ring)]))
        others.append(got)
        for bit in range(1, share):
            others.append(swap(got, bit))

    bounds = lower_bound.reshape(1, width)
    some = 8 if seqs % 8 == 0 else seqs
    one_spec = pl.BlockSpec((1, width), lambda i: (0, 0))
    taken = pl.pallas_call(
        lambda *refs: taken_kernel(*refs, proposals=proposals, seqs=some),
        out_shape=jax.ShapeDtypeStruct(state.shape, F32),
        in_specs=[SMEM, HBM, VMEM, VMEM, VMEM],
        out_specs=HBM,
        scratch_shapes=[
            pltpu.VMEM(state.shape, F32),
            pltpu.SemaphoreType.DMA((seqs // some,)),
            pltpu.SemaphoreType.DMA((seqs // some,)),
        ],
        compiler_params=room(48),
        name="taken",
    )(accepted, state, prev_forget, prev_value, bounds)

    def added(a, b):
        return (a.astype(F32) + b.astype(F32)).astype(BF16)

    tokens_here = []

    def summed(w, weights):
        levels = [1 << k for k in range((ring - 1).bit_length())]
        width = weights[0].shape[1]
        shapes = [jax.ShapeDtypeStruct((rows, width), F32)]
        shapes += [jax.ShapeDtypeStruct((size, rows, width), BF16) for size in levels]
        fresh = w == 0
        if fresh:
            shapes.append(jax.ShapeDtypeStruct((ring * rows, inner * block), BF16))
        operands = [own, *others, *weights] if fresh else [tokens_here[0], *weights]
        products = pl.pallas_call(
            lambda *refs: project_kernel(*refs, ring=ring, inner=inner, share=share, fresh=fresh),
            out_shape=shapes,
            in_specs=[VMEM] * len(operands),
            out_specs=[VMEM] * len(shapes),
            scratch_shapes=[pltpu.VMEM((inner * block, width), BF16)],
            compiler_params=room(16),
            name="project",
        )(*operands)
        if fresh:
            tokens_here.append(products[-1])
        pieces = [products[0]]
        held = {size: products[1 + k] for k, size in enumerate(levels)}
        for size in reversed(levels):
            out = held[size]
            for hop in range(1, size):
                got = lax.ppermute(out, "kv", mirrored(size, hop - 1, hop))
                out = added(out, got)
            got = lax.ppermute(out, "kv", mirrored(size, size - 1, size))
            pieces.append(got)
            for lower in levels:
                if lower < size:
                    start = ((group // lower) ^ 1) * lower % size
                    piece = lax.dynamic_slice_in_dim(got, start, lower, 0)
                    held[lower] = added(held[lower], piece)
        return pieces

    head_parts = [summed(w, weights) for w, weights in enumerate(sets)]

    blocks = []
    cur = w_out[None]
    size, step = 1, 0
    while size < ring:
        got = lax.ppermute(cur, "kv", mirrored(size, size - 1, size))
        step += 1
        total = got
        for hop in range(1, size):
            got = lax.ppermute(got, "kv", mirrored(size, size - hop, size - hop - 1))
            step += 1
            total = total + got
        if size == 1:
            cur = jnp.concatenate([cur, total])
            fresh = cur
        else:
            fresh = total
            if 2 * size < ring:
                cur = jnp.concatenate([cur, total])
        blocks.append(fresh)
        size *= 2
    if ring == 1:
        blocks = [cur]
    weights = []
    for fresh in blocks:
        weights += [fresh] + [lax.ppermute(fresh, "kv", around(t)) for t in range(1, inner)]

    runs = runs_of(heads)
    many = 32 if seqs % 32 == 0 else seqs
    many_rows = many * proposals
    gathered, ids = [], []
    for k, run in enumerate(runs):
        specs, arrays = [], []
        for head in run:
            for array in head_parts[head]:
                arrays.append(array)
                if array.ndim == 2:
                    specs.append(pl.BlockSpec((many_rows, 4 * keys), lambda i: (i, 0)))
                else:
                    specs.append(pl.BlockSpec((array.shape[0], many_rows, 4 * keys), lambda i: (0, i, 0)))
        parts = len(head_parts[0])
        held = len(run)
        place = run[0] // held
        last = k == len(runs) - 1
        head_out = pl.pallas_call(
            lambda *refs, held=held, first=run[0]: recur_kernel(
                *refs, parts=parts, heads=held, first=first, proposals=proposals, inner=inner
            ),
            out_shape=jax.ShapeDtypeStruct((rows, held * keys), BF16),
            grid=(seqs // many,),
            in_specs=specs
            + [pl.BlockSpec((many, held, keys, vals), lambda i, place=place: (i, place, 0, 0)), one_spec, one_spec],
            out_specs=pl.BlockSpec((many_rows, held * keys), lambda i: (i, 0)),
            compiler_params=room(40),
            name="recur",
        )(*arrays, taken, bounds, head_gain.reshape(1, width))
        pieces, ids = [head_out], [0]
        bit = tp // 2
        while bit:
            for j in range(len(ids)):
                if not last:
                    pieces.append(swap(pieces[j], bit))
                else:
                    pieces.append(swap(head_out, ids[j] ^ bit))
            ids += [i ^ bit for i in ids]
            bit //= 2
        gathered += pieces
    table = jnp.asarray(order_of(ring), jnp.int32)
    height = w_out.shape[0]
    mixed = pl.pallas_call(
        lambda *refs: mix_kernel(*refs, lanes=tp, ids=ids, runs=runs, inner=inner, keys=keys),
        out_shape=jax.ShapeDtypeStruct((rows, w_out.shape[1]), BF16),
        in_specs=[SMEM] + [VMEM] * (len(gathered) + len(weights)),
        out_specs=VMEM,
        scratch_shapes=[pltpu.VMEM((kv, rows, height), BF16)],
        compiler_params=room(12),
        name="mix",
    )(table, *gathered, *weights)
    return (mixed, taken)


def cut_of(kv, tp):
    inner = 2 if kv % 2 == 0 else 1
    return inner, kv // inner, 2 if tp % 2 == 0 else 1


def runs_of(heads):
    half = max(1, heads // 2)
    return [list(range(half))] + [[head] for head in range(half, heads)]


def order_of(ring):
    order = [[g] for g in range(ring)]
    size = 1
    while size < ring:
        order = [
            order[g] + order[(g // (2 * size)) * 2 * size + (size if g % (2 * size) < size else size - 1)]
            for g in range(ring)
        ]
        size *= 2
    return np.array(order, np.int32)


def solution(mesh):
    kv, tp = mesh.shape["kv"], mesh.shape["tp"]

    def body(*args):
        return on_device(*args, kv=kv, tp=tp)

    return jax.shard_map(
        body,
        mesh=mesh,
        in_specs=(
            P("kv", None),
            P(),
            P("kv", "tp"),
            P("kv", "tp"),
            P("kv", "tp"),
            P("kv", "tp"),
            P("tp"),
            P("tp"),
            P("kv", "tp"),
            P("kv", "tp", None, None),
            P("kv", None, "tp"),
            P("kv", None, "tp"),
            P("kv"),
        ),
        out_specs=(P("kv", "tp"), P("kv", "tp", None, None)),
        check_vma=False,
    )
```

```python
import jax
import jax.numpy as jnp
import numpy as np
from jax import lax
from jax.experimental import pallas as pl
from jax.experimental.pallas import tpu as pltpu
from jax.sharding import PartitionSpec as P


EPSILON = 1e-06
F32 = jnp.float32
BF16 = jnp.bfloat16
VMEM = pl.BlockSpec(memory_space=pltpu.VMEM)
SMEM = pl.BlockSpec(memory_space=pltpu.SMEM)
HBM = pl.BlockSpec(memory_space=pltpu.MemorySpace.HBM)


def in_hbm(*arrays):
    return [pltpu.with_memory_space_constraint(array, pltpu.MemorySpace.HBM) for array in arrays]


def room(mib):
    return pltpu.CompilerParams(vmem_limit_bytes=mib << 20)


def forget_of(pre_act, bounds):
    return bounds + (1.0 - bounds) * jax.nn.sigmoid(pre_act)


def norm_kernel(tokens, gain, *refs, ring, inner, share, heads):
    weights, own, mine = refs[:4], refs[4], refs[5 : 4 + ring]
    pieces, (raw, scratch, sems, come) = refs[4 + ring : -4], refs[-4:]
    keys = weights[0].shape[1] // heads
    copies = [
        pltpu.make_async_copy(
            weights[k].at[:, pl.ds(head * keys, keys)],
            pieces[head].at[:, pl.ds(k * keys, keys)],
            sems.at[head * 4 + k],
        )
        for head in range(heads)
        for k in range(4)
    ]
    rows, width = tokens.shape
    step = 16
    lots = come.shape[0]
    fetches = [
        pltpu.make_async_copy(tokens.at[here], raw.at[here], come.at[lot])
        for lot in range(lots)
        for here in [pl.ds(lot * (rows // lots), rows // lots)]
    ]
    for copy in fetches + copies:
        copy.start()
    block = own.shape[-1]
    part = rows // share
    chunk = min(width, 512)

    def one(i, carry):
        here = pl.ds(pl.multiple_of(i * step, step), step)
        total = jnp.zeros((step, 128), F32)
        for at in range(0, width, chunk):
            x = raw[here, at : at + chunk].astype(F32)
            x = x * x
            for k in range(0, chunk, 128):
                total = total + x[:, k : k + 128]
        scale = lax.rsqrt(jnp.sum(total, axis=-1, keepdims=True) / width + EPSILON)
        for at in range(0, width, chunk):
            x = raw[here, at : at + chunk].astype(F32)
            scratch[here, at : at + chunk] = (x * scale * gain[:, at : at + chunk]).astype(BF16)
        return carry

    for lot in range(lots):
        fetches[lot].wait()
        first = lot * (rows // lots) // step
        lax.fori_loop(first, first + rows // lots // step, one, 0, unroll=4)
    me, lane = lax.axis_index("kv"), lax.axis_index("tp")
    group, member = lax.div(me, inner), lax.rem(me, inner)
    here = pl.ds(pl.multiple_of(lax.rem(lane, share) * part, part), part)
    for r in range(ring):
        owner = jnp.bitwise_xor(group, r)
        for turn in range(inner):
            column = owner * inner + lax.rem(member + turn, inner)
            cols = pl.ds(pl.multiple_of(column * block, block), block)
            if r == 0:
                own[turn] = scratch[:, cols]
            else:
                mine[r - 1][turn] = scratch[here, cols]
    for copy in copies:
        copy.wait()


def project_kernel(*refs, ring, inner, share, fresh):
    if fresh:
        own, others = refs[0], refs[1 : 1 + (ring - 1) * share]
        weights = refs[1 + (ring - 1) * share :][:inner]
        outs, lhs, stack = refs[1 + (ring - 1) * share + inner : -2], refs[-2], refs[-1]
        rows, block = own.shape[1], own.shape[2]
        part = rows // share
        lane = lax.rem(lax.axis_index("tp"), share)
        for turn in range(inner):
            cols = slice(turn * block, (turn + 1) * block)
            lhs[0:rows, cols] = own[turn]
            for r in range(ring - 1):
                for other in range(share):
                    at = (r + 1) * rows + jnp.bitwise_xor(lane, other) * part
                    lhs[pl.ds(pl.multiple_of(at, part), part), cols] = others[r * share + other][turn]
    else:
        lhs, weights = refs[0], refs[1 : 1 + inner]
        outs, stack = refs[1 + inner : -1], refs[-1]
        block = weights[0].shape[0]
        rows = lhs.shape[0] // ring
    group = lax.div(lax.axis_index("kv"), inner)
    for turn in range(inner):
        stack[turn * block : (turn + 1) * block, :] = weights[turn][...]
    for level in reversed(range(len(outs))):
        size = 1 << max(level - 1, 0)
        start = size if level else 0
        total = jnp.dot(
            lhs[start * rows : (start + size) * rows, :], stack[...], preferred_element_type=F32
        )
        if level:
            for k in range(size):
                at = jnp.bitwise_xor(lax.rem(group, size), k)
                outs[level][at] = total[k * rows : (k + 1) * rows].astype(BF16)
        else:
            outs[0][...] = total


def position_of(shape, proposals):
    return lax.rem(lax.broadcasted_iota(jnp.int32, shape, 0), proposals)


def taken_kernel(
    accepted, state, prev_forget, prev_value, bounds, taken, held, forget, values, come, gone, side, *, proposals, seqs
):
    count, heads, keys, vals = state.shape
    steps = count // seqs
    rows = seqs * proposals
    position = position_of((rows, keys), proposals)
    owner = lax.broadcasted_iota(jnp.int32, (rows, keys), 0) // proposals

    def copy_in(i):
        here = pl.ds(i * seqs, seqs)
        return pltpu.make_async_copy(state.at[here], held.at[here], come.at[i])

    def copy_out(i):
        here = pl.ds(i * seqs, seqs)
        return pltpu.make_async_copy(held.at[here], taken.at[here], gone.at[i])

    fetches = [
        pltpu.make_async_copy(prev_forget, forget, side.at[0]),
        pltpu.make_async_copy(prev_value, values, side.at[1]),
    ]
    for copy in fetches:
        copy.start()
    ahead = min(3, steps)
    for i in range(ahead):
        copy_in(i).start()
    for copy in fetches:
        copy.wait()

    def one(i, carry):
        first = i * seqs

        @pl.when(i + ahead < steps)
        def _():
            copy_in(i + ahead).start()

        old = jnp.concatenate([forget[first + seq].astype(F32) for seq in range(seqs)], axis=0)
        new = jnp.concatenate([values[first + seq].astype(F32) for seq in range(seqs)], axis=0).astype(BF16)
        taking = jnp.zeros((rows, keys), jnp.int32)
        for seq in range(seqs):
            taking = jnp.where(owner == seq, accepted[first + seq], taking)
        kept = position < taking
        decays, addeds = [], []
        for head in range(heads):
            cols = slice(head * keys, (head + 1) * keys)
            gate = forget_of(old[:, cols], bounds[:, cols])
            decay = jnp.where(kept, gate, 1.0)
            after = jnp.ones_like(decay)
            for lead in range(1, proposals):
                moved = pltpu.roll(decay, rows - lead, axis=0)
                after = after * jnp.where(position < proposals - lead, moved, 1.0)
            decays.append((decay * after).T)
            weight = (jnp.where(kept, 1.0 - gate, 0.0) * after).T
            high = weight.astype(BF16)
            low = (weight - high.astype(F32)).astype(BF16)
            value = new[:, head * vals : (head + 1) * vals]
            spread = jnp.concatenate(
                [jnp.where(owner == seq, value, jnp.zeros_like(value)) for seq in range(seqs)], axis=1
            )
            addeds.append(
                jnp.dot(
                    jnp.concatenate([high, low], axis=1),
                    jnp.concatenate([spread, spread], axis=0),
                    preferred_element_type=F32,
                )
            )
        copy_in(i).wait()
        for head in range(heads):
            for seq in range(seqs):
                at = seq * proposals
                held[first + seq, head] = (
                    decays[head][:, at : at + 1] * held[first + seq, head]
                    + addeds[head][:, seq * vals : (seq + 1) * vals]
                )
        copy_out(i).start()
        return carry

    lax.fori_loop(0, steps, one, 0)
    for i in range(steps):
        copy_out(i).wait()


def recur_kernel(*refs, parts, head, proposals, inner, spare):
    pieces, (taken, bounds, gain) = refs[:parts], refs[parts : parts + 3]
    rest = refs[parts + 3 :]
    if spare:
        last, *rest = rest
        *rest, ready = rest
        ready[...] = last[...].astype(BF16)
    out = rest[-1]
    if len(rest) > 1:
        out[:, : rest[0].shape[1]] = rest[0][...]
    where = lax.div(lax.axis_index("kv"), inner)
    seqs, _, keys, vals = taken.shape
    rows = seqs * proposals
    position = position_of((rows, keys), proposals)
    group = 4
    tile = group * proposals
    tile_seq = lax.broadcasted_iota(jnp.int32, (tile, keys), 0) // proposals

    def total_of(k):
        here = slice(k * keys, (k + 1) * keys)
        total = pieces[0][:, here]
        for piece in pieces[1:]:
            total = total + piece[lax.rem(where, piece.shape[0]), :, here].astype(F32)
        return total

    cols = slice(head * keys, (head + 1) * keys)
    gate = forget_of(total_of(0), bounds[:, cols])
    value = total_of(1)
    query = total_of(2) * keys ** (-0.5)
    key = 1.0 - gate
    through = query
    result = jnp.sum(query * key, axis=-1, keepdims=True) * value
    grown = gate
    before = gate
    for lag in range(1, proposals):
        inside = position >= lag
        through = through * jnp.where(inside, before, 0.0)
        score = jnp.sum(through * pltpu.roll(key, lag, axis=0), axis=-1, keepdims=True)
        result = result + score * pltpu.roll(value, lag, axis=0)
        before = pltpu.roll(gate, lag, axis=0)
        grown = grown * jnp.where(inside, before, 1.0)
    reach = (query * grown).astype(BF16)
    met = []
    for at in range(0, seqs, group):
        part = reach[at * proposals : (at + group) * proposals, :]
        lhs = jnp.concatenate(
            [jnp.where(tile_seq == s, part, jnp.zeros_like(part)) for s in range(group)], axis=1
        )
        here = taken[at : at + group, 0].astype(BF16).reshape(group * keys, vals)
        met.append(jnp.dot(lhs, here, preferred_element_type=F32))
    result = result + jnp.concatenate(met, axis=0)
    scale = lax.rsqrt(jnp.mean(result * result, axis=-1, keepdims=True) + EPSILON)
    result = result * scale * gain[:, cols] * jax.nn.silu(total_of(3))
    out[:, out.shape[1] - keys :] = result.astype(BF16)


def mix_kernel(order, *refs, lanes, ids, runs, inner, keys):
    heads, weights = refs[: lanes * len(runs)], refs[lanes * len(runs) : -2]
    out, lhs = refs[-2:]
    height = weights[0].shape[1]
    per = height // keys
    count = sum(len(run) for run in runs)
    mine = lax.axis_index("tp")
    me = lax.axis_index("kv")
    group, member = lax.div(me, inner), lax.rem(me, inner)
    for at, run in enumerate(runs):
        for k, other in enumerate(ids):
            lane = jnp.bitwise_xor(mine, other)
            for j, head in enumerate(run):
                where = lane * (count // per) + head // per
                cols = slice(head % per * keys, (head % per + 1) * keys)
                lhs[where, :, cols] = heads[at * lanes + k][:, j * keys : (j + 1) * keys]
    chunk = min(out.shape[1], 256)
    for n in range(0, out.shape[1], chunk):
        total = None
        slot = 0
        for at in range(0, len(weights), inner):
            for k in range(weights[at].shape[0]):
                for turn in range(inner):
                    place = order[group, slot] * inner + lax.rem(member + turn, inner)
                    product = jnp.dot(
                        lhs[place], weights[at + turn][k, :, n : n + chunk], preferred_element_type=F32
                    )
                    total = product if total is None else total + product
                slot += 1
        out[:, n : n + chunk] = total.astype(out.dtype)


def on_device(
    tokens,
    norm_gain,
    w_query,
    w_forget,
    w_value,
    w_gate,
    lower_bound,
    head_gain,
    w_out,
    state,
    prev_forget,
    prev_value,
    accepted,
    *,
    kv,
    tp,
):
    seqs, heads, keys, vals = state.shape
    proposals = prev_forget.shape[1]
    rows = tokens.shape[0]
    width = heads * keys
    inner, ring, share = cut_of(kv, tp)

    group = lax.axis_index("kv") // inner

    def groups(pairs):
        return [(a * inner + m, b * inner + m) for a, b in pairs for m in range(inner)]

    def around(turn):
        return [(g * inner + (m + turn) % inner, g * inner + m) for g in range(ring) for m in range(inner)]

    def mirrored(size, start, stop):
        pairs = []
        for base in range(0, ring, 2 * size):
            last = base + 2 * size - 1
            pairs += [(base + start, base + stop), (last - start, last - stop)]
        return groups(pairs)

    def swap(value, bit):
        return lax.ppermute(value, "tp", [(t, t ^ bit) for t in range(tp)])

    block = w_query.shape[0]
    part = rows // share
    shapes = [jax.ShapeDtypeStruct((inner, rows, block), BF16)]
    shapes += [jax.ShapeDtypeStruct((inner, part, block), BF16)] * (ring - 1)
    shapes += [jax.ShapeDtypeStruct((block, 4 * keys), BF16)] * heads
    normed = pl.pallas_call(
        lambda *refs: norm_kernel(*refs, ring=ring, inner=inner, share=share, heads=heads),
        out_shape=shapes,
        in_specs=[HBM, VMEM] + [HBM] * 4,
        out_specs=[VMEM] * len(shapes),
        scratch_shapes=[
            pltpu.VMEM(tokens.shape, BF16),
            pltpu.VMEM(tokens.shape, BF16),
            pltpu.SemaphoreType.DMA((4 * heads,)),
            pltpu.SemaphoreType.DMA((4 if rows % 256 == 0 else 1,)),
        ],
        compiler_params=room(16),
        name="norm",
    )(*in_hbm(tokens, norm_gain.reshape(1, -1), w_forget, w_value, w_query, w_gate))
    own, mine = normed[0], normed[1:ring]
    sets = []
    for weight in normed[ring:]:
        sets.append([weight] + [lax.ppermute(weight, "kv", around(t)) for t in range(1, inner)])
    others = []
    for r in range(1, ring):
        got = lax.ppermute(mine[r - 1], "kv", groups([(g, g ^ r) for g in range(ring)]))
        others.append(got)
        for bit in range(1, share):
            others.append(swap(got, bit))

    bounds = lower_bound.reshape(1, width)
    some = 8 if seqs % 8 == 0 else seqs
    one_spec = pl.BlockSpec((1, width), lambda i: (0, 0))
    taken = pl.pallas_call(
        lambda *refs: taken_kernel(*refs, proposals=proposals, seqs=some),
        out_shape=jax.ShapeDtypeStruct(state.shape, F32),
        in_specs=[SMEM, HBM, HBM, HBM, VMEM],
        out_specs=HBM,
        scratch_shapes=[
            pltpu.VMEM(state.shape, F32),
            pltpu.VMEM(prev_forget.shape, BF16),
            pltpu.VMEM(prev_value.shape, BF16),
            pltpu.SemaphoreType.DMA((seqs // some,)),
            pltpu.SemaphoreType.DMA((seqs // some,)),
            pltpu.SemaphoreType.DMA((2,)),
        ],
        compiler_params=room(24),
        name="taken",
    )(*in_hbm(accepted, state, prev_forget, prev_value, bounds))

    def added(a, b):
        return (a.astype(F32) + b.astype(F32)).astype(BF16)

    tokens_here = []

    def summed(w, weights):
        levels = [1 << k for k in range((ring - 1).bit_length())]
        width = weights[0].shape[1]
        shapes = [jax.ShapeDtypeStruct((rows, width), F32)]
        shapes += [jax.ShapeDtypeStruct((size, rows, width), BF16) for size in levels]
        fresh = w == 0
        if fresh:
            shapes.append(jax.ShapeDtypeStruct((ring * rows, inner * block), BF16))
        operands = [own, *others, *weights] if fresh else [tokens_here[0], *weights]
        products = pl.pallas_call(
            lambda *refs: project_kernel(*refs, ring=ring, inner=inner, share=share, fresh=fresh),
            out_shape=shapes,
            in_specs=[VMEM] * len(operands),
            out_specs=[VMEM] * len(shapes),
            scratch_shapes=[pltpu.VMEM((inner * block, width), BF16)],
            compiler_params=room(16),
            name="project",
        )(*operands)
        if fresh:
            tokens_here.append(products[-1])
        pieces = [products[0]]
        held = {size: products[1 + k] for k, size in enumerate(levels)}
        for size in reversed(levels):
            out = held[size]
            for hop in range(1, size):
                got = lax.ppermute(out, "kv", mirrored(size, hop - 1, hop))
                out = added(out, got)
            got = lax.ppermute(out, "kv", mirrored(size, size - 1, size))
            pieces.append(got)
            for lower in levels:
                if lower < size:
                    start = ((group // lower) ^ 1) * lower % size
                    piece = lax.dynamic_slice_in_dim(got, start, lower, 0)
                    held[lower] = added(held[lower], piece)
        return pieces

    head_parts = [summed(w, weights) for w, weights in enumerate(sets)]

    blocks = []
    cur = w_out[None]
    size, step = 1, 0
    while size < ring:
        got = lax.ppermute(cur, "kv", mirrored(size, size - 1, size))
        step += 1
        total = got
        for hop in range(1, size):
            got = lax.ppermute(got, "kv", mirrored(size, size - hop, size - hop - 1))
            step += 1
            total = total + got
        if size == 1:
            cur = jnp.concatenate([cur, total])
            fresh = cur
        else:
            fresh = total
            if 2 * size < ring:
                cur = jnp.concatenate([cur, total])
        blocks.append(fresh)
        size *= 2
    if ring == 1:
        blocks = [cur]
    weights = []
    for fresh in blocks:
        weights += [fresh] + [lax.ppermute(fresh, "kv", around(t)) for t in range(1, inner)]

    runs = runs_of(heads)
    many = 32 if seqs % 32 == 0 else seqs
    many_rows = many * proposals
    parts = len(head_parts[0])
    gathered, ids = [], []
    ready = None
    for k, run in enumerate(runs):
        last = k == len(runs) - 1
        head_out = None
        for head in run:
            spare = head == 0 and heads > 1
            source = in_hbm(taken)[0] if ready is None or head < heads - 1 else ready
            arrays = [*head_parts[head], source, bounds, head_gain.reshape(1, width)]

            def spec_of(array):
                if array.ndim == 2:
                    return pl.BlockSpec((many_rows, array.shape[1]), lambda i: (i, 0))
                return pl.BlockSpec((array.shape[0], many_rows, array.shape[2]), lambda i: (0, i, 0))

            def state_of(index):
                return pl.BlockSpec((many, 1, keys, vals), lambda i: (i, index, 0, 0))

            specs = [spec_of(array) for array in head_parts[head]]
            specs += [state_of(0 if source is ready else head), one_spec, one_spec]
            cols = keys
            shapes = []
            if spare:
                arrays.append(in_hbm(taken)[0])
                specs.append(state_of(heads - 1))
            if head_out is not None:
                arrays.append(head_out)
                specs.append(spec_of(head_out))
                cols += head_out.shape[1]
            shapes.append(jax.ShapeDtypeStruct((rows, cols), BF16))
            outs = [pl.BlockSpec((many_rows, cols), lambda i: (i, 0))]
            if spare:
                shapes.append(jax.ShapeDtypeStruct((seqs, 1, keys, vals), BF16))
                outs.append(state_of(0))
            head_out, *more = pl.pallas_call(
                lambda *refs, head=head, spare=spare: recur_kernel(
                    *refs, parts=parts, head=head, proposals=proposals, inner=inner, spare=spare
                ),
                out_shape=shapes,
                grid=(seqs // many,),
                in_specs=specs,
                out_specs=outs,
                compiler_params=room(20),
                name="recur",
            )(*arrays)
            if spare:
                ready = more[0]
        pieces, ids = [head_out], [0]
        bit = tp // 2
        while bit:
            for j in range(len(ids)):
                if not last:
                    pieces.append(swap(pieces[j], bit))
                else:
                    pieces.append(swap(head_out, ids[j] ^ bit))
            ids += [i ^ bit for i in ids]
            bit //= 2
        gathered += pieces
    table = jnp.asarray(order_of(ring), jnp.int32)
    height = w_out.shape[0]
    mixed = pl.pallas_call(
        lambda *refs: mix_kernel(*refs, lanes=tp, ids=ids, runs=runs, inner=inner, keys=keys),
        out_shape=jax.ShapeDtypeStruct((rows, w_out.shape[1]), BF16),
        in_specs=[SMEM] + [VMEM] * (len(gathered) + len(weights)),
        out_specs=VMEM,
        scratch_shapes=[pltpu.VMEM((kv, rows, height), BF16)],
        compiler_params=room(12),
        name="mix",
    )(table, *gathered, *weights)
    return (mixed, taken)


def cut_of(kv, tp):
    inner = 2 if kv % 2 == 0 else 1
    return inner, kv // inner, 2 if tp % 2 == 0 else 1


def runs_of(heads):
    return [list(range(heads - 1)), [heads - 1]] if heads > 1 else [[0]]


def order_of(ring):
    order = [[g] for g in range(ring)]
    size = 1
    while size < ring:
        order = [
            order[g] + order[(g // (2 * size)) * 2 * size + (size if g % (2 * size) < size else size - 1)]
            for g in range(ring)
        ]
        size *= 2
    return np.array(order, np.int32)


def solution(mesh):
    kv, tp = mesh.shape["kv"], mesh.shape["tp"]

    def body(*args):
        return on_device(*args, kv=kv, tp=tp)

    return jax.shard_map(
        body,
        mesh=mesh,
        in_specs=(
            P("kv", None),
            P(),
            P("kv", "tp"),
            P("kv", "tp"),
            P("kv", "tp"),
            P("kv", "tp"),
            P("tp"),
            P("tp"),
            P("kv", "tp"),
            P("kv", "tp", None, None),
            P("kv", None, "tp"),
            P("kv", None, "tp"),
            P("kv"),
        ),
        out_specs=(P("kv", "tp"), P("kv", "tp", None, None)),
        check_vma=False,
    )
```

```python
import jax
import jax.numpy as jnp
import numpy as np
from jax import lax
from jax.experimental import pallas as pl
from jax.experimental.pallas import tpu as pltpu
from jax.sharding import PartitionSpec as P


EPSILON = 1e-06
F32 = jnp.float32
BF16 = jnp.bfloat16
VMEM = pl.BlockSpec(memory_space=pltpu.VMEM)
SMEM = pl.BlockSpec(memory_space=pltpu.SMEM)
HBM = pl.BlockSpec(memory_space=pltpu.MemorySpace.HBM)


def in_hbm(*arrays):
    return [pltpu.with_memory_space_constraint(array, pltpu.MemorySpace.HBM) for array in arrays]


def room(mib):
    return pltpu.CompilerParams(vmem_limit_bytes=mib << 20)


def forget_of(pre_act, bounds):
    return bounds + (1.0 - bounds) * jax.nn.sigmoid(pre_act)


def norm_kernel(tokens, gain, *refs, ring, inner, share, heads):
    weights, own, mine = refs[:4], refs[4], refs[5 : 4 + ring]
    pieces, (raw, scratch, sems, come) = refs[4 + ring : -4], refs[-4:]
    keys = weights[0].shape[1] // heads
    copies = [
        pltpu.make_async_copy(
            weights[k].at[:, pl.ds(head * keys, keys)],
            pieces[head].at[:, pl.ds(k * keys, keys)],
            sems.at[head * 4 + k],
        )
        for head in range(heads)
        for k in range(4)
    ]
    rows, width = tokens.shape
    step = 16
    lots = come.shape[0]
    fetches = [
        pltpu.make_async_copy(tokens.at[here], raw.at[here], come.at[lot])
        for lot in range(lots)
        for here in [pl.ds(lot * (rows // lots), rows // lots)]
    ]
    for copy in fetches + copies:
        copy.start()
    block = own.shape[-1]
    part = rows // share
    chunk = min(width, 512)

    def one(i, carry):
        here = pl.ds(pl.multiple_of(i * step, step), step)
        total = jnp.zeros((step, 128), F32)
        for at in range(0, width, chunk):
            x = raw[here, at : at + chunk].astype(F32)
            x = x * x
            for k in range(0, chunk, 128):
                total = total + x[:, k : k + 128]
        scale = lax.rsqrt(jnp.sum(total, axis=-1, keepdims=True) / width + EPSILON)
        for at in range(0, width, chunk):
            x = raw[here, at : at + chunk].astype(F32)
            scratch[here, at : at + chunk] = (x * scale * gain[:, at : at + chunk]).astype(BF16)
        return carry

    for lot in range(lots):
        fetches[lot].wait()
        first = lot * (rows // lots) // step
        lax.fori_loop(first, first + rows // lots // step, one, 0, unroll=4)
    me, lane = lax.axis_index("kv"), lax.axis_index("tp")
    group, member = lax.div(me, inner), lax.rem(me, inner)
    here = pl.ds(pl.multiple_of(lax.rem(lane, share) * part, part), part)
    for r in range(ring):
        owner = jnp.bitwise_xor(group, r)
        for turn in range(inner):
            column = owner * inner + lax.rem(member + turn, inner)
            cols = pl.ds(pl.multiple_of(column * block, block), block)
            if r == 0:
                own[turn] = scratch[:, cols]
            else:
                mine[r - 1][turn] = scratch[here, cols]
    for copy in copies:
        copy.wait()


def project_kernel(*refs, ring, inner, share, fresh):
    if fresh:
        own, others = refs[0], refs[1 : 1 + (ring - 1) * share]
        weights = refs[1 + (ring - 1) * share :][:inner]
        outs, lhs, stack = refs[1 + (ring - 1) * share + inner : -2], refs[-2], refs[-1]
        rows, block = own.shape[1], own.shape[2]
        part = rows // share
        lane = lax.rem(lax.axis_index("tp"), share)
        for turn in range(inner):
            cols = slice(turn * block, (turn + 1) * block)
            lhs[0:rows, cols] = own[turn]
            for r in range(ring - 1):
                for other in range(share):
                    at = (r + 1) * rows + jnp.bitwise_xor(lane, other) * part
                    lhs[pl.ds(pl.multiple_of(at, part), part), cols] = others[r * share + other][turn]
    else:
        lhs, weights = refs[0], refs[1 : 1 + inner]
        outs, stack = refs[1 + inner : -1], refs[-1]
        block = weights[0].shape[0]
        rows = lhs.shape[0] // ring
    group = lax.div(lax.axis_index("kv"), inner)
    for turn in range(inner):
        stack[turn * block : (turn + 1) * block, :] = weights[turn][...]
    for level in reversed(range(len(outs))):
        size = 1 << max(level - 1, 0)
        start = size if level else 0
        total = jnp.dot(
            lhs[start * rows : (start + size) * rows, :], stack[...], preferred_element_type=F32
        )
        if level:
            for k in range(size):
                at = jnp.bitwise_xor(lax.rem(group, size), k)
                outs[level][at] = total[k * rows : (k + 1) * rows].astype(BF16)
        else:
            outs[0][...] = total


def position_of(shape, proposals):
    return lax.rem(lax.broadcasted_iota(jnp.int32, shape, 0), proposals)


def taken_kernel(
    accepted, state, prev_forget, prev_value, bounds, *refs, proposals, seqs, start
):
    taken, held, forget, values, come, gone, side = refs[-7:]
    count, heads, keys, vals = held.shape
    steps = count // seqs
    rows = seqs * proposals
    position = position_of((rows, keys), proposals)
    owner = lax.broadcasted_iota(jnp.int32, (rows, keys), 0) // proposals

    def copy_in(i):
        here = pl.ds(i * seqs, seqs)
        return pltpu.make_async_copy(state.at[pl.ds(start + i * seqs, seqs)], held.at[here], come.at[i])

    def copy_out(i):
        here = pl.ds(i * seqs, seqs)
        return pltpu.make_async_copy(held.at[here], taken.at[pl.ds(start + i * seqs, seqs)], gone.at[i])

    fetches = [
        pltpu.make_async_copy(prev_forget.at[pl.ds(start, count)], forget, side.at[0]),
        pltpu.make_async_copy(prev_value.at[pl.ds(start, count)], values, side.at[1]),
    ]
    for copy in fetches:
        copy.start()
    ahead = min(2, steps)
    for i in range(ahead):
        copy_in(i).start()
    for copy in fetches:
        copy.wait()

    def one(i, carry):
        first = i * seqs

        @pl.when(i + ahead < steps)
        def _():
            copy_in(i + ahead).start()

        old = jnp.concatenate([forget[first + seq].astype(F32) for seq in range(seqs)], axis=0)
        new = jnp.concatenate([values[first + seq].astype(F32) for seq in range(seqs)], axis=0).astype(BF16)
        taking = jnp.zeros((rows, keys), jnp.int32)
        for seq in range(seqs):
            taking = jnp.where(owner == seq, accepted[start + first + seq], taking)
        kept = position < taking
        decays, addeds = [], []
        for head in range(heads):
            cols = slice(head * keys, (head + 1) * keys)
            gate = forget_of(old[:, cols], bounds[:, cols])
            decay = jnp.where(kept, gate, 1.0)
            after = jnp.ones_like(decay)
            for lead in range(1, proposals):
                moved = pltpu.roll(decay, rows - lead, axis=0)
                after = after * jnp.where(position < proposals - lead, moved, 1.0)
            decays.append((decay * after).T)
            weight = (jnp.where(kept, 1.0 - gate, 0.0) * after).T
            high = weight.astype(BF16)
            low = (weight - high.astype(F32)).astype(BF16)
            value = new[:, head * vals : (head + 1) * vals]
            spread = jnp.concatenate(
                [jnp.where(owner == seq, value, jnp.zeros_like(value)) for seq in range(seqs)], axis=1
            )
            addeds.append(
                jnp.dot(
                    jnp.concatenate([high, low], axis=1),
                    jnp.concatenate([spread, spread], axis=0),
                    preferred_element_type=F32,
                )
            )
        copy_in(i).wait()
        for head in range(heads):
            for seq in range(seqs):
                at = seq * proposals
                held[first + seq, head] = (
                    decays[head][:, at : at + 1] * held[first + seq, head]
                    + addeds[head][:, seq * vals : (seq + 1) * vals]
                )
        copy_out(i).start()
        return carry

    lax.fori_loop(0, steps, one, 0)
    for i in range(steps):
        copy_out(i).wait()


def recur_kernel(*refs, parts, head, proposals, inner, spare):
    pieces, (taken, bounds, gain) = refs[:parts], refs[parts : parts + 3]
    rest = refs[parts + 3 :]
    if spare:
        last, *rest = rest
        *rest, ready = rest
        ready[...] = last[...].astype(BF16)
    out = rest[-1]
    if len(rest) > 1:
        out[:, : rest[0].shape[1]] = rest[0][...]
    where = lax.div(lax.axis_index("kv"), inner)
    seqs, _, keys, vals = taken.shape
    rows = seqs * proposals
    position = position_of((rows, keys), proposals)
    group = 4
    tile = group * proposals
    tile_seq = lax.broadcasted_iota(jnp.int32, (tile, keys), 0) // proposals

    def total_of(k):
        here = slice(k * keys, (k + 1) * keys)
        total = pieces[0][:, here]
        for piece in pieces[1:]:
            total = total + piece[lax.rem(where, piece.shape[0]), :, here].astype(F32)
        return total

    cols = slice(head * keys, (head + 1) * keys)
    gate = forget_of(total_of(0), bounds[:, cols])
    value = total_of(1)
    query = total_of(2) * keys ** (-0.5)
    key = 1.0 - gate
    through = query
    result = jnp.sum(query * key, axis=-1, keepdims=True) * value
    grown = gate
    before = gate
    for lag in range(1, proposals):
        inside = position >= lag
        through = through * jnp.where(inside, before, 0.0)
        score = jnp.sum(through * pltpu.roll(key, lag, axis=0), axis=-1, keepdims=True)
        result = result + score * pltpu.roll(value, lag, axis=0)
        before = pltpu.roll(gate, lag, axis=0)
        grown = grown * jnp.where(inside, before, 1.0)
    reach = (query * grown).astype(BF16)
    met = []
    for at in range(0, seqs, group):
        part = reach[at * proposals : (at + group) * proposals, :]
        lhs = jnp.concatenate(
            [jnp.where(tile_seq == s, part, jnp.zeros_like(part)) for s in range(group)], axis=1
        )
        here = taken[at : at + group, 0].astype(BF16).reshape(group * keys, vals)
        met.append(jnp.dot(lhs, here, preferred_element_type=F32))
    result = result + jnp.concatenate(met, axis=0)
    scale = lax.rsqrt(jnp.mean(result * result, axis=-1, keepdims=True) + EPSILON)
    result = result * scale * gain[:, cols] * jax.nn.silu(total_of(3))
    out[:, out.shape[1] - keys :] = result.astype(BF16)


def mix_kernel(order, *refs, lanes, ids, runs, inner, keys):
    heads, weights = refs[: lanes * len(runs)], refs[lanes * len(runs) : -2]
    out, lhs = refs[-2:]
    height = weights[0].shape[1]
    per = height // keys
    count = sum(len(run) for run in runs)
    mine = lax.axis_index("tp")
    me = lax.axis_index("kv")
    group, member = lax.div(me, inner), lax.rem(me, inner)
    for at, run in enumerate(runs):
        for k, other in enumerate(ids):
            lane = jnp.bitwise_xor(mine, other)
            for j, head in enumerate(run):
                where = lane * (count // per) + head // per
                cols = slice(head % per * keys, (head % per + 1) * keys)
                lhs[where, :, cols] = heads[at * lanes + k][:, j * keys : (j + 1) * keys]
    chunk = min(out.shape[1], 256)
    for n in range(0, out.shape[1], chunk):
        total = None
        slot = 0
        for at in range(0, len(weights), inner):
            for k in range(weights[at].shape[0]):
                for turn in range(inner):
                    place = order[group, slot] * inner + lax.rem(member + turn, inner)
                    product = jnp.dot(
                        lhs[place], weights[at + turn][k, :, n : n + chunk], preferred_element_type=F32
                    )
                    total = product if total is None else total + product
                slot += 1
        out[:, n : n + chunk] = total.astype(out.dtype)


def on_device(
    tokens,
    norm_gain,
    w_query,
    w_forget,
    w_value,
    w_gate,
    lower_bound,
    head_gain,
    w_out,
    state,
    prev_forget,
    prev_value,
    accepted,
    *,
    kv,
    tp,
):
    seqs, heads, keys, vals = state.shape
    proposals = prev_forget.shape[1]
    rows = tokens.shape[0]
    width = heads * keys
    inner, ring, share = cut_of(kv, tp)

    group = lax.axis_index("kv") // inner

    def groups(pairs):
        return [(a * inner + m, b * inner + m) for a, b in pairs for m in range(inner)]

    def around(turn):
        return [(g * inner + (m + turn) % inner, g * inner + m) for g in range(ring) for m in range(inner)]

    def mirrored(size, start, stop):
        pairs = []
        for base in range(0, ring, 2 * size):
            last = base + 2 * size - 1
            pairs += [(base + start, base + stop), (last - start, last - stop)]
        return groups(pairs)

    def swap(value, bit):
        return lax.ppermute(value, "tp", [(t, t ^ bit) for t in range(tp)])

    block = w_query.shape[0]
    part = rows // share
    shapes = [jax.ShapeDtypeStruct((inner, rows, block), BF16)]
    shapes += [jax.ShapeDtypeStruct((inner, part, block), BF16)] * (ring - 1)
    shapes += [jax.ShapeDtypeStruct((block, 4 * keys), BF16)] * heads
    normed = pl.pallas_call(
        lambda *refs: norm_kernel(*refs, ring=ring, inner=inner, share=share, heads=heads),
        out_shape=shapes,
        in_specs=[HBM, VMEM] + [HBM] * 4,
        out_specs=[VMEM] * len(shapes),
        scratch_shapes=[
            pltpu.VMEM(tokens.shape, BF16),
            pltpu.VMEM(tokens.shape, BF16),
            pltpu.SemaphoreType.DMA((4 * heads,)),
            pltpu.SemaphoreType.DMA((4 if rows % 256 == 0 else 1,)),
        ],
        compiler_params=room(16),
        name="norm",
    )(*in_hbm(tokens, norm_gain.reshape(1, -1), w_forget, w_value, w_query, w_gate))
    own, mine = normed[0], normed[1:ring]
    sets = []
    for weight in normed[ring:]:
        sets.append([weight] + [lax.ppermute(weight, "kv", around(t)) for t in range(1, inner)])
    others = []
    for r in range(1, ring):
        got = lax.ppermute(mine[r - 1], "kv", groups([(g, g ^ r) for g in range(ring)]))
        others.append(got)
        for bit in range(1, share):
            others.append(swap(got, bit))

    bounds = lower_bound.reshape(1, width)
    some = 8 if seqs % 8 == 0 else seqs
    one_spec = pl.BlockSpec((1, width), lambda i: (0, 0))
    steps = seqs // some
    middle = max(1, steps * 5 // 8)
    taken = None
    for first, last in [(0, middle), (middle, steps)]:
        if first == last:
            continue
        done = [] if taken is None else [taken]
        span = (last - first) * some
        taken = pl.pallas_call(
            lambda *refs, start=first * some: taken_kernel(*refs, proposals=proposals, seqs=some, start=start),
            out_shape=jax.ShapeDtypeStruct(state.shape, F32),
            in_specs=[SMEM, HBM, HBM, HBM, VMEM] + [HBM] * len(done),
            out_specs=HBM,
            input_output_aliases={5: 0} if done else {},
            scratch_shapes=[
                pltpu.VMEM((span, *state.shape[1:]), F32),
                pltpu.VMEM((span, *prev_forget.shape[1:]), BF16),
                pltpu.VMEM((span, *prev_value.shape[1:]), BF16),
                pltpu.SemaphoreType.DMA((last - first,)),
                pltpu.SemaphoreType.DMA((last - first,)),
                pltpu.SemaphoreType.DMA((2,)),
            ],
            compiler_params=room(24),
            name="taken",
        )(*in_hbm(accepted, state, prev_forget, prev_value, bounds, *done))

    def added(a, b):
        return (a.astype(F32) + b.astype(F32)).astype(BF16)

    tokens_here = []

    def summed(w, weights):
        levels = [1 << k for k in range((ring - 1).bit_length())]
        width = weights[0].shape[1]
        shapes = [jax.ShapeDtypeStruct((rows, width), F32)]
        shapes += [jax.ShapeDtypeStruct((size, rows, width), BF16) for size in levels]
        fresh = w == 0
        if fresh:
            shapes.append(jax.ShapeDtypeStruct((ring * rows, inner * block), BF16))
        operands = [own, *others, *weights] if fresh else [tokens_here[0], *weights]
        products = pl.pallas_call(
            lambda *refs: project_kernel(*refs, ring=ring, inner=inner, share=share, fresh=fresh),
            out_shape=shapes,
            in_specs=[VMEM] * len(operands),
            out_specs=[VMEM] * len(shapes),
            scratch_shapes=[pltpu.VMEM((inner * block, width), BF16)],
            compiler_params=room(16),
            name="project",
        )(*operands)
        if fresh:
            tokens_here.append(products[-1])
        pieces = [products[0]]
        held = {size: products[1 + k] for k, size in enumerate(levels)}
        for size in reversed(levels):
            out = held[size]
            for hop in range(1, size):
                got = lax.ppermute(out, "kv", mirrored(size, hop - 1, hop))
                out = added(out, got)
            got = lax.ppermute(out, "kv", mirrored(size, size - 1, size))
            pieces.append(got)
            for lower in levels:
                if lower < size:
                    start = ((group // lower) ^ 1) * lower % size
                    piece = lax.dynamic_slice_in_dim(got, start, lower, 0)
                    held[lower] = added(held[lower], piece)
        return pieces

    head_parts = [summed(w, weights) for w, weights in enumerate(sets)]

    blocks = []
    cur = w_out[None]
    size, step = 1, 0
    while size < ring:
        got = lax.ppermute(cur, "kv", mirrored(size, size - 1, size))
        step += 1
        total = got
        for hop in range(1, size):
            got = lax.ppermute(got, "kv", mirrored(size, size - hop, size - hop - 1))
            step += 1
            total = total + got
        if size == 1:
            cur = jnp.concatenate([cur, total])
            fresh = cur
        else:
            fresh = total
            if 2 * size < ring:
                cur = jnp.concatenate([cur, total])
        blocks.append(fresh)
        size *= 2
    if ring == 1:
        blocks = [cur]
    weights = []
    for fresh in blocks:
        weights += [fresh] + [lax.ppermute(fresh, "kv", around(t)) for t in range(1, inner)]

    runs = runs_of(heads)
    many = 32 if seqs % 32 == 0 else seqs
    many_rows = many * proposals
    parts = len(head_parts[0])
    gathered, ids = [], []
    ready = None
    for k, run in enumerate(runs):
        last = k == len(runs) - 1
        head_out = None
        for head in run:
            spare = head == 0 and heads > 1
            source = in_hbm(taken)[0] if ready is None or head < heads - 1 else ready
            arrays = [*head_parts[head], source, bounds, head_gain.reshape(1, width)]

            def spec_of(array):
                if array.ndim == 2:
                    return pl.BlockSpec((many_rows, array.shape[1]), lambda i: (i, 0))
                return pl.BlockSpec((array.shape[0], many_rows, array.shape[2]), lambda i: (0, i, 0))

            def state_of(index):
                return pl.BlockSpec((many, 1, keys, vals), lambda i: (i, index, 0, 0))

            specs = [spec_of(array) for array in head_parts[head]]
            specs += [state_of(0 if source is ready else head), one_spec, one_spec]
            cols = keys
            shapes = []
            if spare:
                arrays.append(in_hbm(taken)[0])
                specs.append(state_of(heads - 1))
            if head_out is not None:
                arrays.append(head_out)
                specs.append(spec_of(head_out))
                cols += head_out.shape[1]
            shapes.append(jax.ShapeDtypeStruct((rows, cols), BF16))
            outs = [pl.BlockSpec((many_rows, cols), lambda i: (i, 0))]
            if spare:
                shapes.append(jax.ShapeDtypeStruct((seqs, 1, keys, vals), BF16))
                outs.append(state_of(0))
            head_out, *more = pl.pallas_call(
                lambda *refs, head=head, spare=spare: recur_kernel(
                    *refs, parts=parts, head=head, proposals=proposals, inner=inner, spare=spare
                ),
                out_shape=shapes,
                grid=(seqs // many,),
                in_specs=specs,
                out_specs=outs,
                compiler_params=room(20),
                name="recur",
            )(*arrays)
            if spare:
                ready = more[0]
        pieces, ids = [head_out], [0]
        bit = tp // 2
        while bit:
            for j in range(len(ids)):
                if not last:
                    pieces.append(swap(pieces[j], bit))
                else:
                    pieces.append(swap(head_out, ids[j] ^ bit))
            ids += [i ^ bit for i in ids]
            bit //= 2
        gathered += pieces
    table = jnp.asarray(order_of(ring), jnp.int32)
    height = w_out.shape[0]
    mixed = pl.pallas_call(
        lambda *refs: mix_kernel(*refs, lanes=tp, ids=ids, runs=runs, inner=inner, keys=keys),
        out_shape=jax.ShapeDtypeStruct((rows, w_out.shape[1]), BF16),
        in_specs=[SMEM] + [VMEM] * (len(gathered) + len(weights)),
        out_specs=VMEM,
        scratch_shapes=[pltpu.VMEM((kv, rows, height), BF16)],
        compiler_params=room(12),
        name="mix",
    )(table, *gathered, *weights)
    return (mixed, taken)


def cut_of(kv, tp):
    inner = 2 if kv % 2 == 0 else 1
    return inner, kv // inner, 2 if tp % 2 == 0 else 1


def runs_of(heads):
    return [list(range(heads - 1)), [heads - 1]] if heads > 1 else [[0]]


def order_of(ring):
    order = [[g] for g in range(ring)]
    size = 1
    while size < ring:
        order = [
            order[g] + order[(g // (2 * size)) * 2 * size + (size if g % (2 * size) < size else size - 1)]
            for g in range(ring)
        ]
        size *= 2
    return np.array(order, np.int32)


def solution(mesh):
    kv, tp = mesh.shape["kv"], mesh.shape["tp"]

    def body(*args):
        return on_device(*args, kv=kv, tp=tp)

    return jax.shard_map(
        body,
        mesh=mesh,
        in_specs=(
            P("kv", None),
            P(),
            P("kv", "tp"),
            P("kv", "tp"),
            P("kv", "tp"),
            P("kv", "tp"),
            P("tp"),
            P("tp"),
            P("kv", "tp"),
            P("kv", "tp", None, None),
            P("kv", None, "tp"),
            P("kv", None, "tp"),
            P("kv"),
        ),
        out_specs=(P("kv", "tp"), P("kv", "tp", None, None)),
        check_vma=False,
    )
```
